128 devices in a mesh: ep: 64 (over z, y, x), tp: 2 (over core).
Axes of the slice: x: 4, y: 4, z: 4, core: 2. Of those that a mesh axis runs over, the one named last changes fastest.
Arguments:
- tokens: bfloat16 [2048, 3072], P('ep'), may hold values from -6 to 6
- carried: float32 [2048, 96, 128], P('ep', 'tp'), may hold values from -4 to 4
- decay_rate: float32 [96, 64], P('tp'), may hold values from 0.02 to 20
- frequency: float32 [96, 64], P('tp'), may hold values from 0 to 200
- log_step: float32 [96], P('tp'), may hold values from -4.6 to 0
- in_map: bfloat16 [96, 128, 16], P('tp'), may hold values from -1 to 1
- out_map: bfloat16 [96, 16, 128], P('tp'), may hold values from -0.5 to 0.5
- skip_gain: float32 [1536], P('tp'), may hold values from -4 to 4
- norm_gain: float32 [3072], replicated, may hold values from 0.1 to 1.9
- w_in: bfloat16 [3072, 1536], P(None, 'tp'), may hold values from -0.109375 to 0.109375
- w_out: bfloat16 [1536, 3072], P('tp'), may hold values from -0.15625 to 0.15625
- expert_gain: float32 [3072], replicated, may hold values from 0.1 to 1.9
- route_ids: int32 [2048, 2], P('ep'), may hold values from 0 to 7, all different within a row; in each aligned block of 32 rows (0 to 31, 32 to 63, ...) at most 16 rows name the same one
- route_logit: float32 [2048, 2], P('ep'), may hold values from -6 to 6
- w_gate: bfloat16 [3072, 43008], P(None, ('ep', 'tp')), may hold values from -0.109375 to 0.109375
- w_up: bfloat16 [3072, 43008], P(None, ('ep', 'tp')), may hold values from -0.109375 to 0.109375
- w_down: bfloat16 [43008, 3072], P(('ep', 'tp')), may hold values from -0.078125 to 0.078125
Outputs:
- new_tokens: bfloat16 [2048, 3072], P('ep', 'tp')
- new_carried: float32 [2048, 96, 128], P('ep', 'tp')
The draws below stay inside these ranges and needn't reach their ends.
Inputs may be any that keep to these rules, and one draw needn't show every extreme that they name: `route_ids`: each row names 2 different experts; within each aligned block of 32 rows (the rows of one index of ep) no expert is named by more than 16 rows, a bound that some block reaches.
All inputs are finite; a program needn't handle non-finite values.
Results may differ from the reference program's by a relative error of at most 0.014.
Values may be sent and summed in bfloat16 or wider, within the bound.
No kernel may reach another device: no remote copies, remote signals or barrier semaphores. Data moves between devices by JAX's collectives and lax.ppermute only.
A program may use at most 128 MiB of HBM per device.

```python
import math
import jax
import jax.numpy as jnp
import numpy as np
from jax import lax

D = 3072
GROUPS = 96
CH = 16
STATE = 64
FF = 5376
EXPERTS = 8
TOP = 2
SEQ_DEV = 32
SEQS = 2048
WIDTH = 1536
CAP = 16
N_TP = 2


def block_scale(rng, dims, split, low, largest):
    loudness, own = 1.0, jax.random.fold_in(rng, 6)
    for dim, shards_of in split:
        steps = jnp.exp(jax.random.uniform(jax.random.fold_in(own, dim), (shards_of,), jnp.float32, low / len(split), largest / len(split)))
        loudness = loudness * jnp.repeat(steps, dims[dim] // shards_of).reshape([-1 if axis == dim else 1 for axis in range(len(dims))])
    return loudness


def shared_out(key, own, number, rows, amount, top, most, slope):
    ranking = jax.random.permutation(key, amount)
    heavy_load, usual = load_shares(amount, rows * top, most, slope, True), load_shares(amount, rows * top, most, slope, False)
    places = jnp.arange(amount)

    def named(sizes, turn):
        used = int((sizes > 0).sum())
        fixed = max(1, used // 4)
        moved = fixed + (places - fixed + turn * (used - fixed)) % max(1, amount - fixed)
        return jnp.zeros((amount,), jnp.int32).at[ranking[jnp.where(places < fixed, places, moved)]].set(jnp.asarray(sizes, jnp.int32))

    sizes = jnp.where(number % 4 == 0, named(heavy_load, number // 4), named(usual, number - number // 4 - 1))
    mixed = jax.random.permutation(jax.random.fold_in(own, 3), amount)
    giver, sink = mixed[0:amount // 2 * 2:2], mixed[1:amount // 2 * 2:2]
    slack = jnp.minimum(sizes[giver] - 1, most - sizes[sink]) // 2
    slack = jnp.where((giver == ranking[0]) | (sink == ranking[0]) | (sizes[sink] == 0), 0, jnp.maximum(slack, 0))
    moved = jax.random.randint(jax.random.fold_in(own, 4), (amount // 2,), 0, 1 << 20) % (slack + 1)
    sizes = sizes.at[giver].add(-moved).at[sink].add(moved)
    members = jnp.searchsorted(jnp.cumsum(sizes), jnp.arange(rows * top), side="right").astype(jnp.int32)
    grid = members.reshape(top, rows).T
    grid = grid[jax.random.permutation(jax.random.fold_in(own, 1), rows)]
    turn = jax.random.randint(jax.random.fold_in(own, 2), (rows, 1), 0, top)
    return jnp.take_along_axis(grid, (jnp.arange(top)[None, :] + turn) % top, axis=1)


def load_shares(amount, total, limit, slope, full):
    loads = [(1 << 20) // math.isqrt(standing ** slope) + 1 for standing in range(1, amount + 1)]
    largest = limit if full else min(limit, max(-(-total // amount), total * loads[0] // sum(loads)))
    least = 1 if total - largest >= amount - 1 else 0
    holding, rest = [largest] + [least] * (amount - 1), total - largest - least * (amount - 1)
    while rest > 0:
        movable = [i for i in range(1, amount) if holding[i] < largest] or [i for i in range(1, amount) if holding[i] < limit]
        whole, budget = sum([loads[i] for i in movable]), rest
        for i in movable:
            extra = min(limit - holding[i], max(1, budget * loads[i] // whole), rest)
            holding[i] = holding[i] + extra
            rest = rest - extra
    return np.array(holding)


def gaussian(stream_key, dims, scale, bound, cuts=(), dtype=jnp.bfloat16):
    level = block_scale(stream_key, dims, cuts, -0.22, 0.18) if cuts else 1.0
    array = jax.random.normal(stream_key, dims, jnp.float32) * scale * level
    return jnp.minimum(jnp.maximum(array, -bound), bound).astype(dtype)


def setup_inputs(seed: int = 0) -> dict:
    arg_keys = jax.random.split(jax.random.key(seed), 18)
    tokens = gaussian(arg_keys[0], (SEQS, D), 1.0, 6.0, ((0, 64),))
    carried = gaussian(arg_keys[1], (SEQS, GROUPS, 2 * STATE), 0.5, 4.0, ((0, 64), (1, 2)), jnp.float32)
    decay_rate = jnp.clip(jnp.exp(math.log(20.0) - 6.9077553 * jax.random.uniform(arg_keys[2], (GROUPS, STATE), jnp.float32) ** block_scale(arg_keys[2], (GROUPS, STATE), ((0, 2),), -0.2, 0.2)), 0.02, 20.0)
    frequency = jnp.clip(200.0 * jax.random.uniform(arg_keys[3], (GROUPS, STATE), jnp.float32) ** block_scale(arg_keys[3], (GROUPS, STATE), ((0, 2),), -0.2, 0.2), 0.0, 200.0)
    log_step = jnp.clip(-4.6 + 4.6 * jax.random.uniform(arg_keys[4], (GROUPS,), jnp.float32) ** block_scale(arg_keys[4], (GROUPS,), ((0, 2),), -0.2, 0.2), -4.6, 0.0)
    in_map = gaussian(arg_keys[5], (GROUPS, 2 * STATE, CH), (2 * CH) ** -0.5, 1.0, ((0, 2),))
    out_map = gaussian(arg_keys[6], (GROUPS, CH, 2 * STATE), (2 * STATE) ** -0.5, 0.5, ((0, 2),))
    skip_gain = gaussian(arg_keys[7], (WIDTH,), 1.0, 4.0, ((0, 2),), jnp.float32)
    norm_gain = jnp.clip(1.0 + 0.18 * jax.random.normal(arg_keys[8], (D,), jnp.float32), 0.1, 1.9)
    w_in = gaussian(arg_keys[9], (D, WIDTH), D ** -0.5, 0.109375, ((1, 2),))
    w_out = gaussian(arg_keys[10], (WIDTH, D), WIDTH ** -0.5, 0.15625, ((0, 2),))
    expert_gain = jnp.clip(1.0 + 0.18 * jax.random.normal(arg_keys[11], (D,), jnp.float32), 0.1, 1.9)
    route_ids_keys = jax.random.split(jax.random.fold_in(arg_keys[12], 1), SEQS // SEQ_DEV)
    route_ids_turns = jax.random.permutation(jax.random.fold_in(arg_keys[12], 3), SEQS // SEQ_DEV)
    route_ids = jax.vmap(lambda own, number: shared_out(jax.random.fold_in(arg_keys[12], 2), own, number, SEQ_DEV, EXPERTS, TOP, CAP, 1))(route_ids_keys, route_ids_turns).reshape((SEQS, TOP))
    route_logit = gaussian(arg_keys[13], (SEQS, TOP), 1.5, 6.0, ((0, 64),), jnp.float32)
    w_gate = gaussian(arg_keys[14], (D, EXPERTS * FF), D ** -0.5, 0.109375, ((1, 128),))
    w_up = gaussian(arg_keys[15], (D, EXPERTS * FF), D ** -0.5, 0.109375, ((1, 128),))
    w_down = gaussian(arg_keys[16], (EXPERTS * FF, D), FF ** -0.5, 0.078125, ((0, 128),))
    return dict(tokens=tokens, carried=carried, decay_rate=decay_rate, frequency=frequency, log_step=log_step, in_map=in_map, out_map=out_map, skip_gain=skip_gain, norm_gain=norm_gain, w_in=w_in, w_out=w_out, expert_gain=expert_gain, route_ids=route_ids, route_logit=route_logit, w_gate=w_gate, w_up=w_up, w_down=w_down)


def normalize(rows, gain):
    wide = rows.astype(jnp.float32)
    scaled = wide * lax.rsqrt(lax.optimization_barrier(jnp.mean(wide * wide, axis=-1, keepdims=True)) + 1e-06)
    return (scaled * gain).astype(jnp.bfloat16)

def state_update(drive, carried, decay_rate, frequency, log_step, in_map, out_map, skip_gain):
    count_rows, width = drive.shape
    groups, half = decay_rate.shape
    channels = width // groups
    step_size = jnp.exp(log_step)[:, None]
    magnitude = jnp.exp(-decay_rate * step_size)
    real_decay = magnitude * jnp.cos(frequency * step_size)
    imag_decay = magnitude * jnp.sin(frequency * step_size)
    denom = decay_rate * decay_rate + frequency * frequency
    real_less = real_decay - 1.0
    real_factor = (-real_less * decay_rate + imag_decay * frequency) / denom
    imag_factor = (-imag_decay * decay_rate - real_less * frequency) / denom
    wide_drive = drive.astype(jnp.float32).reshape(count_rows, groups, channels)
    projected = jnp.einsum('sgh,gqh->sgq', wide_drive, in_map.astype(jnp.float32))
    real_in = projected[..., :half]
    imag_in = projected[..., half:]
    real_push = real_factor * real_in - imag_factor * imag_in
    imag_push = real_factor * imag_in + imag_factor * real_in
    real_old = carried[..., :half]
    imag_old = carried[..., half:]
    real_new = real_decay * real_old - imag_decay * imag_old + real_push
    imag_new = real_decay * imag_old + imag_decay * real_old + imag_push
    joined = jnp.concatenate([real_new, -imag_new], axis=-1)
    reading = jnp.einsum('sgq,ghq->sgh', joined, out_map.astype(jnp.float32), precision=lax.Precision.HIGHEST)
    total = reading.reshape(count_rows, width) + skip_gain * drive.astype(jnp.float32)
    activated = jax.nn.gelu(total).astype(jnp.bfloat16)
    return (activated, jnp.concatenate([real_new, imag_new], axis=-1))

def route_weights(route_logit):
    first = jax.nn.sigmoid(route_logit[:, 0] - route_logit[:, 1])
    second = jax.nn.sigmoid(route_logit[:, 1] - route_logit[:, 0])
    return jnp.stack([first, second], axis=1)

def expert_output(rows, gate_cols, up_cols, down_rows):
    gated = jnp.dot(rows, gate_cols, preferred_element_type=jnp.float32)
    upward = jnp.dot(rows, up_cols, preferred_element_type=jnp.float32)
    hidden = (jax.nn.silu(gated) * upward).astype(jnp.bfloat16)
    return jnp.dot(hidden, down_rows, preferred_element_type=jnp.float32)

def reference(tokens, carried, decay_rate, frequency, log_step, in_map, out_map, skip_gain, norm_gain, w_in, w_out, expert_gain, route_ids, route_logit, w_gate, w_up, w_down):
    normed = normalize(tokens, norm_gain)
    drive = jnp.dot(normed, w_in, preferred_element_type=jnp.float32).astype(jnp.bfloat16)
    activated, new_carried = state_update(drive, carried, decay_rate, frequency, log_step, in_map, out_map, skip_gain)
    block = activated.shape[1] // N_TP
    summed = jnp.zeros(tokens.shape, jnp.float32)
    for index in range(N_TP):
        partial_value = jnp.dot(activated[:, index * block:(index + 1) * block], w_out[index * block:(index + 1) * block], preferred_element_type=jnp.float32).astype(jnp.bfloat16)
        summed = summed + partial_value.astype(jnp.float32)
    mixed = (tokens.astype(jnp.float32) + summed).astype(jnp.bfloat16)
    expert_in = normalize(mixed, expert_gain)
    weights = route_weights(route_logit)
    hidden_units = w_gate.shape[1] // EXPERTS
    total = mixed.astype(jnp.float32)
    for expert in range(EXPERTS):
        chosen = lax.optimization_barrier(jnp.sum(jnp.where(route_ids == expert, weights, 0.0), axis=1))
        lower = expert * hidden_units
        upper = lower + hidden_units
        produced = expert_output(expert_in, w_gate[:, lower:upper], w_up[:, lower:upper], w_down[lower:upper])
        total = total + chosen[:, None] * produced
    return (total.astype(jnp.bfloat16), new_carried)
```

```python
import jax
import jax.numpy as jnp
from jax import lax
from jax.sharding import PartitionSpec as P

EXPERTS = 8
TOP = 2
CAP = 16


def swapped(shard):
    return lax.ppermute(shard, "tp", [(0, 1), (1, 0)])


def normalize(rows, gain):
    wide = rows.astype(jnp.float32)
    scaled = wide * lax.rsqrt(jnp.mean(wide * wide, axis=-1, keepdims=True) + 1e-06)
    return (scaled * gain).astype(jnp.bfloat16)


def state_update(drive, carried, decay_rate, frequency, log_step, in_map, out_map, skip_gain):
    count_rows, width = drive.shape
    groups, half = decay_rate.shape
    channels = width // groups
    step_size = jnp.exp(log_step)[:, None]
    magnitude = jnp.exp(-decay_rate * step_size)
    real_decay = magnitude * jnp.cos(frequency * step_size)
    imag_decay = magnitude * jnp.sin(frequency * step_size)
    denom = decay_rate * decay_rate + frequency * frequency
    real_less = real_decay - 1.0
    real_factor = (-real_less * decay_rate + imag_decay * frequency) / denom
    imag_factor = (-imag_decay * decay_rate - real_less * frequency) / denom
    grouped_drive = drive.reshape(count_rows, groups, channels)
    projected = jnp.einsum(
        "sgh,gqh->sgq", grouped_drive, in_map, preferred_element_type=jnp.float32
    )
    real_in = projected[..., :half]
    imag_in = projected[..., half:]
    real_push = real_factor * real_in - imag_factor * imag_in
    imag_push = real_factor * imag_in + imag_factor * real_in
    real_old = carried[..., :half]
    imag_old = carried[..., half:]
    real_new = real_decay * real_old - imag_decay * imag_old + real_push
    imag_new = real_decay * imag_old + imag_decay * real_old + imag_push
    joined = jnp.concatenate([real_new, -imag_new], axis=-1)
    reading = jnp.einsum("sgq,ghq->sgh", joined, out_map.astype(jnp.float32))
    total = reading.reshape(count_rows, width) + skip_gain * drive.astype(jnp.float32)
    activated = jax.nn.gelu(total).astype(jnp.bfloat16)
    return (activated, jnp.concatenate([real_new, imag_new], axis=-1))


def route_weights(route_logit):
    first = jax.nn.sigmoid(route_logit[:, 0] - route_logit[:, 1])
    second = jax.nn.sigmoid(route_logit[:, 1] - route_logit[:, 0])
    return jnp.stack([first, second], axis=1)


def per_device(
    tokens,
    carried,
    decay_rate,
    frequency,
    log_step,
    in_map,
    out_map,
    skip_gain,
    norm_gain,
    w_in,
    w_out,
    expert_gain,
    route_ids,
    route_logit,
    w_gate,
    w_up,
    w_down,
):
    count_rows, model_width = tokens.shape
    core = lax.axis_index("tp")
    group_size = lax.axis_size("ep") // EXPERTS
    slots = CAP // lax.axis_size("tp")
    normed = normalize(tokens, norm_gain)
    drive = jnp.dot(normed, w_in, preferred_element_type=jnp.float32).astype(jnp.bfloat16)
    activated, new_carried = state_update(
        drive, carried, decay_rate, frequency, log_step, in_map, out_map, skip_gain
    )
    partial_value = jnp.dot(activated, w_out, preferred_element_type=jnp.float32).astype(
        jnp.bfloat16
    )
    summed = partial_value.astype(jnp.float32) + swapped(partial_value).astype(jnp.float32)
    mixed = (tokens.astype(jnp.float32) + summed).astype(jnp.bfloat16)
    expert_in = normalize(mixed, expert_gain)
    weights = route_weights(route_logit)
    gate_both = jnp.concatenate([w_gate, swapped(w_gate)], axis=1)
    up_both = jnp.concatenate([w_up, swapped(w_up)], axis=1)
    down_both = jnp.concatenate([w_down, swapped(w_down)], axis=0)
    expert_ids = jnp.arange(EXPERTS, dtype=jnp.int32)
    routes_flat = route_ids.reshape(-1)
    weights_flat = weights.reshape(-1)
    onehot = (routes_flat[:, None] == expert_ids[None, :]).astype(jnp.int32)
    earlier = jnp.cumsum(onehot, axis=0) - onehot
    slot_index = jnp.sum(earlier * onehot, axis=1) - core * slots
    held = (slot_index >= 0) & (slot_index < slots)
    position = jnp.where(held, routes_flat * slots + slot_index, -1)
    placement = (
        jnp.arange(EXPERTS * slots, dtype=jnp.int32)[:, None] == position[None, :]
    ).astype(jnp.float32)
    per_token = placement.reshape(EXPERTS * slots, count_rows, TOP).sum(axis=2)
    packed = jnp.dot(per_token.astype(jnp.bfloat16), expert_in, preferred_element_type=jnp.float32)
    packed = packed.astype(jnp.bfloat16).reshape(EXPERTS, slots, model_width)
    outgoing = jnp.repeat(packed, group_size, axis=0)
    received = lax.all_to_all(outgoing, "ep", split_axis=0, concat_axis=0, tiled=True)
    rows = received.reshape(-1, model_width)
    gated = jnp.dot(rows, gate_both, preferred_element_type=jnp.float32)
    upward = jnp.dot(rows, up_both, preferred_element_type=jnp.float32)
    hidden = (jax.nn.silu(gated) * upward).astype(jnp.bfloat16)
    produced = jnp.dot(hidden, down_both, preferred_element_type=jnp.float32)
    produced = produced.astype(jnp.bfloat16).reshape(received.shape)
    returned = lax.all_to_all(produced, "ep", split_axis=0, concat_axis=0, tiled=True)
    per_expert = returned.reshape(EXPERTS, group_size, slots, -1).astype(jnp.float32).sum(axis=1)
    per_expert = per_expert.reshape(EXPERTS * slots, -1)
    weighing = (
        (placement * weights_flat[None, :]).reshape(EXPERTS * slots, count_rows, TOP).sum(axis=2)
    )
    expert_sum = jnp.dot(weighing.T, per_expert, preferred_element_type=jnp.float32)
    half_width = model_width // lax.axis_size("tp")
    own_sum = lax.dynamic_slice_in_dim(expert_sum, core * half_width, half_width, 1)
    other_sum = lax.dynamic_slice_in_dim(expert_sum, (1 - core) * half_width, half_width, 1)
    own_mixed = lax.dynamic_slice_in_dim(mixed, core * half_width, half_width, 1)
    new_tokens = (own_mixed.astype(jnp.float32) + (own_sum + swapped(other_sum))).astype(
        jnp.bfloat16
    )
    return (new_tokens, new_carried)


def solution(mesh):
    return jax.shard_map(
        per_device,
        mesh=mesh,
        in_specs=(
            P("ep", None),
            P("ep", "tp", None),
            P("tp", None),
            P("tp", None),
            P("tp"),
            P("tp", None, None),
            P("tp", None, None),
            P("tp"),
            P(),
            P(None, "tp"),
            P("tp", None),
            P(),
            P("ep", None),
            P("ep", None),
            P(None, ("ep", "tp")),
            P(None, ("ep", "tp")),
            P(("ep", "tp"), None),
        ),
        out_specs=(P("ep", "tp"), P("ep", "tp", None)),
        check_vma=False,
    )
```

```python
import jax
import jax.numpy as jnp
from jax import lax
from jax.sharding import PartitionSpec as P

EXPERTS = 8
TOP = 2
CAP = 16
Y_SIZE = 4
X_SIZE = 4
SELECT = ("za", "zb", "yb")
SPREAD = ("ya", "xa", "xb")
COLOURS = ((0, 3), (3, 6), (6, 8))


def gray(value):
    return value ^ (value >> 1)


def neighbour(chip, link):
    place = {"z": chip // (Y_SIZE * X_SIZE), "y": chip // X_SIZE % Y_SIZE, "x": chip % X_SIZE}
    axis, bit = link
    code = gray(place[axis]) ^ (1 if bit == "a" else 2)
    place[axis] = code ^ (code >> 1)
    return (place["z"] * Y_SIZE + place["y"]) * X_SIZE + place["x"]


def over_link(shard, links):
    pairs = [
        (chip * 2 + core, neighbour(chip, links[core]) * 2 + core)
        for chip in range(lax.axis_size("ep"))
        for core in range(2)
    ]
    return lax.ppermute(shard, ("ep", "tp"), pairs)


def select_links(step):
    return (SELECT[step], SELECT[(step + 1) % 3])


def spread_links(step, colour):
    link = SPREAD[(step + colour) % 3]
    return (link, link)


def swapped(shard):
    return lax.ppermute(shard, "tp", [(0, 1), (1, 0)])


def normalize(rows, gain):
    wide = rows.astype(jnp.float32)
    scaled = wide * lax.rsqrt(jnp.mean(wide * wide, axis=-1, keepdims=True) + 1e-06)
    return (scaled * gain).astype(jnp.bfloat16)


def state_update(drive, carried, decay_rate, frequency, log_step, in_map, out_map, skip_gain):
    count_rows, width = drive.shape
    groups, half = decay_rate.shape
    channels = width // groups
    step_size = jnp.exp(log_step)[:, None]
    magnitude = jnp.exp(-decay_rate * step_size)
    real_decay = magnitude * jnp.cos(frequency * step_size)
    imag_decay = magnitude * jnp.sin(frequency * step_size)
    denom = decay_rate * decay_rate + frequency * frequency
    real_less = real_decay - 1.0
    real_factor = (-real_less * decay_rate + imag_decay * frequency) / denom
    imag_factor = (-imag_decay * decay_rate - real_less * frequency) / denom
    grouped_drive = drive.reshape(count_rows, groups, channels)
    projected = jnp.einsum(
        "sgh,gqh->sgq", grouped_drive, in_map, preferred_element_type=jnp.float32
    )
    real_in = projected[..., :half]
    imag_in = projected[..., half:]
    real_push = real_factor * real_in - imag_factor * imag_in
    imag_push = real_factor * imag_in + imag_factor * real_in
    real_old = carried[..., :half]
    imag_old = carried[..., half:]
    real_new = real_decay * real_old - imag_decay * imag_old + real_push
    imag_new = real_decay * imag_old + imag_decay * real_old + imag_push
    joined = jnp.concatenate([real_new, -imag_new], axis=-1)
    reading = jnp.einsum("sgq,ghq->sgh", joined, out_map.astype(jnp.float32))
    total = reading.reshape(count_rows, width) + skip_gain * drive.astype(jnp.float32)
    activated = jax.nn.gelu(total).astype(jnp.bfloat16)
    return (activated, jnp.concatenate([real_new, imag_new], axis=-1))


def route_weights(route_logit):
    first = jax.nn.sigmoid(route_logit[:, 0] - route_logit[:, 1])
    second = jax.nn.sigmoid(route_logit[:, 1] - route_logit[:, 0])
    return jnp.stack([first, second], axis=1)


def per_device(
    tokens,
    carried,
    decay_rate,
    frequency,
    log_step,
    in_map,
    out_map,
    skip_gain,
    norm_gain,
    w_in,
    w_out,
    expert_gain,
    route_ids,
    route_logit,
    w_gate,
    w_up,
    w_down,
):
    count_rows, model_width = tokens.shape
    core = lax.axis_index("tp")
    slots = CAP // lax.axis_size("tp")
    normed = normalize(tokens, norm_gain)
    drive = jnp.dot(normed, w_in, preferred_element_type=jnp.float32).astype(jnp.bfloat16)
    activated, new_carried = state_update(
        drive, carried, decay_rate, frequency, log_step, in_map, out_map, skip_gain
    )
    partial_value = jnp.dot(activated, w_out, preferred_element_type=jnp.float32).astype(
        jnp.bfloat16
    )
    summed = partial_value.astype(jnp.float32) + swapped(partial_value).astype(jnp.float32)
    mixed = (tokens.astype(jnp.float32) + summed).astype(jnp.bfloat16)
    expert_in = normalize(mixed, expert_gain)
    weights = route_weights(route_logit)
    gate_both = jnp.concatenate([w_gate, swapped(w_gate)], axis=1)
    up_both = jnp.concatenate([w_up, swapped(w_up)], axis=1)
    down_both = jnp.concatenate([w_down, swapped(w_down)], axis=0)
    chip = lax.axis_index("ep")
    own_z, own_y = chip // (Y_SIZE * X_SIZE), chip // X_SIZE % Y_SIZE
    expert_z, expert_y = route_ids // 2, route_ids % 2
    differ = (gray(expert_z) ^ gray(own_z), expert_y ^ (own_y >> 1))
    bit_za, bit_zb, bit_yb = differ[0] & 1, differ[0] >> 1, differ[1]
    block = jnp.where(
        core == 0,
        bit_za * 4 + bit_zb * 2 + bit_yb,
        bit_zb * 4 + bit_yb * 2 + bit_za,
    ).reshape(-1)
    expert_ids = jnp.arange(EXPERTS, dtype=jnp.int32)
    routes_flat = route_ids.reshape(-1)
    weights_flat = weights.reshape(-1)
    onehot = (routes_flat[:, None] == expert_ids[None, :]).astype(jnp.int32)
    earlier = jnp.cumsum(onehot, axis=0) - onehot
    slot_index = jnp.sum(earlier * onehot, axis=1) - core * slots
    held = (slot_index >= 0) & (slot_index < slots)
    position = jnp.where(held, block * slots + slot_index, -1)
    placement = (
        jnp.arange(EXPERTS * slots, dtype=jnp.int32)[:, None] == position[None, :]
    ).astype(jnp.float32)
    per_token = placement.reshape(EXPERTS * slots, count_rows, TOP).sum(axis=2)
    packed = jnp.dot(per_token.astype(jnp.bfloat16), expert_in, preferred_element_type=jnp.float32)
    blocks = packed.astype(jnp.bfloat16).reshape(2, 2, 2, slots, model_width)
    for step in range(3):
        came = over_link(blocks[1], select_links(step))
        blocks = jnp.stack([blocks[0], came], axis=-3)
    gathered = blocks.reshape(EXPERTS, slots, model_width)
    gathered, gate_both, up_both, down_both, new_carried = lax.optimization_barrier(
        (gathered, gate_both, up_both, down_both, new_carried)
    )
    sums = []
    for colour, (first, last) in enumerate(COLOURS):
        rows = gathered[first:last].reshape(-1, model_width)
        for step in range(3):
            rows = jnp.concatenate([rows, over_link(rows, spread_links(step, colour))], axis=0)
        gated = jnp.dot(rows, gate_both, preferred_element_type=jnp.float32)
        upward = jnp.dot(rows, up_both, preferred_element_type=jnp.float32)
        hidden = (jax.nn.silu(gated) * upward).astype(jnp.bfloat16)
        total = jnp.dot(hidden, down_both, preferred_element_type=jnp.float32)
        for step in (2, 1, 0):
            half = total.shape[0] // 2
            came = over_link(total[half:].astype(jnp.bfloat16), spread_links(step, colour))
            total = total[:half] + came.astype(jnp.float32)
        sums.append(total.astype(jnp.bfloat16))
    blocks = jnp.concatenate(sums, axis=0).reshape(2, 2, 2, slots, model_width)
    for step in (2, 1, 0):
        came = over_link(blocks[:, :, 1], select_links(step))
        blocks = jnp.stack([blocks[:, :, 0], came], axis=0)
    per_expert = blocks.reshape(EXPERTS * slots, model_width).astype(jnp.float32)
    weighing = (
        (placement * weights_flat[None, :]).reshape(EXPERTS * slots, count_rows, TOP).sum(axis=2)
    )
    expert_sum = jnp.dot(weighing.T, per_expert, preferred_element_type=jnp.float32)
    half_width = model_width // lax.axis_size("tp")
    own_sum = lax.dynamic_slice_in_dim(expert_sum, core * half_width, half_width, 1)
    other_sum = lax.dynamic_slice_in_dim(expert_sum, (1 - core) * half_width, half_width, 1)
    own_mixed = lax.dynamic_slice_in_dim(mixed, core * half_width, half_width, 1)
    new_tokens = (own_mixed.astype(jnp.float32) + (own_sum + swapped(other_sum))).astype(
        jnp.bfloat16
    )
    return (new_tokens, new_carried)


def solution(mesh):
    return jax.shard_map(
        per_device,
        mesh=mesh,
        in_specs=(
            P("ep", None),
            P("ep", "tp", None),
            P("tp", None),
            P("tp", None),
            P("tp"),
            P("tp", None, None),
            P("tp", None, None),
            P("tp"),
            P(),
            P(None, "tp"),
            P("tp", None),
            P(),
            P("ep", None),
            P("ep", None),
            P(None, ("ep", "tp")),
            P(None, ("ep", "tp")),
            P(("ep", "tp"), None),
        ),
        out_specs=(P("ep", "tp"), P("ep", "tp", None)),
        check_vma=False,
    )
```

```python
import jax
import jax.numpy as jnp
from jax import lax
from jax.experimental import pallas as pl
from jax.experimental.pallas import tpu as pltpu
from jax.sharding import PartitionSpec as P

EXPERTS = 8
TOP = 2
CAP = 16
Y_SIZE = 4
X_SIZE = 4
SELECT = ("za", "zb", "yb")
SPREAD = ("ya", "xa", "xb")
COLOURS = ((0, 3), (3, 6), (6, 8))
OUT_CHUNK = 512


def gray(value):
    return value ^ (value >> 1)


def neighbour(chip, link):
    place = {"z": chip // (Y_SIZE * X_SIZE), "y": chip // X_SIZE % Y_SIZE, "x": chip % X_SIZE}
    axis, bit = link
    code = gray(place[axis]) ^ (1 if bit == "a" else 2)
    place[axis] = code ^ (code >> 1)
    return (place["z"] * Y_SIZE + place["y"]) * X_SIZE + place["x"]


def over_links(shard, links):
    pairs = []
    for chip in range(lax.axis_size("ep")):
        other = chip
        for link in links:
            other = neighbour(other, link)
        pairs += [(chip * 2 + core, other * 2 + core) for core in range(2)]
    return lax.ppermute(shard, ("ep", "tp"), pairs)


def select_links(block):
    return [link for bit, link in zip((4, 2, 1), SELECT) if block & bit]


def spread_links(step, colour):
    return [SPREAD[(step + colour) % 3]]


def swapped(shard):
    return lax.ppermute(shard, "tp", [(0, 1), (1, 0)])


def unit_cuts(units):
    cuts = []
    for first in range(0, 2 * units, 256):
        last = min(first + 256, 2 * units)
        copies = []
        for which in range(2):
            low, high = max(first, which * units), min(last, (which + 1) * units)
            if low < high:
                copies.append((which, low - which * units, low, high - low))
        cuts.append((first, last - first, copies))
    return cuts


def expert_kernel(sizes, units, *refs):
    count = len(sizes)
    pieces, refs = refs[:count], refs[count:]
    gates, ups, downs, refs = refs[0:2], refs[2:4], refs[4:6], refs[6:]
    outs, refs = refs[:count], refs[count:]
    rows, gate, up, down, hidden, result, row_sem, unit_sem, down_sem, out_sem = refs
    starts = [sum(sizes[:index]) for index in range(count)]
    row_copies = [
        pltpu.make_async_copy(piece, rows.at[pl.ds(start, size)], row_sem.at[index])
        for index, (piece, start, size) in enumerate(zip(pieces, starts, sizes))
    ]
    cuts = unit_cuts(units)
    unit_copies = []
    number = 0
    for _, _, copies in cuts:
        chunk = []
        for which, source, target, size in copies:
            for weights, held in ((gates, gate), (ups, up)):
                chunk.append(
                    pltpu.make_async_copy(
                        weights[which].at[pl.ds(source, size)],
                        held.at[pl.ds(target, size)],
                        unit_sem.at[number],
                    )
                )
                number += 1
        unit_copies.append(chunk)
    down_copies = [
        pltpu.make_async_copy(
            downs[which], down.at[pl.ds(which * units, units)], down_sem.at[which]
        )
        for which in range(2)
    ]
    for copy in unit_copies[0] + row_copies + unit_copies[1]:
        copy.start()
    for copy in row_copies:
        copy.wait()
    contract = (((1,), (1,)), ((), ()))
    for index, (first, size, _) in enumerate(cuts):
        for copy in unit_copies[index]:
            copy.wait()
        if index + 2 < len(cuts):
            for copy in unit_copies[index + 2]:
                copy.start()
        if index + 2 == len(cuts):
            for copy in down_copies:
                copy.start()
        span = pl.ds(first, size)
        gated = lax.dot_general(
            rows[...], gate[span, :], contract, preferred_element_type=jnp.float32
        )
        upward = lax.dot_general(
            rows[...], up[span, :], contract, preferred_element_type=jnp.float32
        )
        hidden[:, span] = (jax.nn.silu(gated) * upward).astype(hidden.dtype)
    for copy in down_copies:
        copy.wait()
    out_copies = []
    for step in range(result.shape[1] // OUT_CHUNK):
        span = pl.ds(step * OUT_CHUNK, OUT_CHUNK)
        result[:, span] = jnp.dot(
            hidden[...], down[:, span], preferred_element_type=jnp.float32
        ).astype(result.dtype)
        for index, (out, start, size) in enumerate(zip(outs, starts, sizes)):
            copy = pltpu.make_async_copy(
                result.at[pl.ds(start, size), span], out.at[:, span], out_sem.at[step, index]
            )
            copy.start()
            out_copies.append(copy)
    for copy in out_copies:
        copy.wait()


def experts(pieces, gates, ups, downs, dtype):
    sizes = [piece.shape[0] for piece in pieces]
    units, width = gates[0].shape
    count_rows = sum(sizes)
    copies = 2 * sum(len(cut[2]) for cut in unit_cuts(units))
    whole = pl.BlockSpec(memory_space=pl.ANY)
    held = pltpu.VMEM((2 * units, width), jnp.bfloat16)
    return pl.pallas_call(
        lambda *refs: expert_kernel(sizes, units, *refs),
        out_shape=[jax.ShapeDtypeStruct((size, width), dtype) for size in sizes],
        in_specs=[whole] * (len(pieces) + 6),
        out_specs=[whole] * len(pieces),
        scratch_shapes=[
            pltpu.VMEM((count_rows, width), jnp.bfloat16),
            held,
            held,
            held,
            pltpu.VMEM((count_rows, 2 * units), jnp.bfloat16),
            pltpu.VMEM((count_rows, width), dtype),
            pltpu.SemaphoreType.DMA((len(pieces),)),
            pltpu.SemaphoreType.DMA((copies,)),
            pltpu.SemaphoreType.DMA((2,)),
            pltpu.SemaphoreType.DMA((width // OUT_CHUNK, len(pieces))),
        ],
        compiler_params=pltpu.CompilerParams(vmem_limit_bytes=40 * 1024 * 1024),
        cost_estimate=pl.CostEstimate(
            flops=12 * count_rows * units * width,
            transcendentals=2 * count_rows * units,
            bytes_accessed=12 * units * width + 4 * count_rows * width,
        ),
        name="experts",
    )(*pieces, *gates, *ups, *downs)


def normalize(rows, gain):
    wide = rows.astype(jnp.float32)
    scaled = wide * lax.rsqrt(jnp.mean(wide * wide, axis=-1, keepdims=True) + 1e-06)
    return (scaled * gain).astype(jnp.bfloat16)


def state_update(drive, carried, decay_rate, frequency, log_step, in_map, out_map, skip_gain):
    count_rows, width = drive.shape
    groups, half = decay_rate.shape
    channels = width // groups
    step_size = jnp.exp(log_step)[:, None]
    magnitude = jnp.exp(-decay_rate * step_size)
    real_decay = magnitude * jnp.cos(frequency * step_size)
    imag_decay = magnitude * jnp.sin(frequency * step_size)
    denom = decay_rate * decay_rate + frequency * frequency
    real_less = real_decay - 1.0
    real_factor = (-real_less * decay_rate + imag_decay * frequency) / denom
    imag_factor = (-imag_decay * decay_rate - real_less * frequency) / denom
    grouped_drive = drive.reshape(count_rows, groups, channels)
    projected = jnp.einsum(
        "sgh,gqh->sgq", grouped_drive, in_map, preferred_element_type=jnp.float32
    )
    real_in = projected[..., :half]
    imag_in = projected[..., half:]
    real_push = real_factor * real_in - imag_factor * imag_in
    imag_push = real_factor * imag_in + imag_factor * real_in
    real_old = carried[..., :half]
    imag_old = carried[..., half:]
    real_new = real_decay * real_old - imag_decay * imag_old + real_push
    imag_new = real_decay * imag_old + imag_decay * real_old + imag_push
    joined = jnp.concatenate([real_new, -imag_new], axis=-1)
    reading = jnp.einsum("sgq,ghq->sgh", joined, out_map.astype(jnp.float32))
    total = reading.reshape(count_rows, width) + skip_gain * drive.astype(jnp.float32)
    activated = jax.nn.gelu(total).astype(jnp.bfloat16)
    return (activated, jnp.concatenate([real_new, imag_new], axis=-1))


def route_weights(route_logit):
    first = jax.nn.sigmoid(route_logit[:, 0] - route_logit[:, 1])
    second = jax.nn.sigmoid(route_logit[:, 1] - route_logit[:, 0])
    return jnp.stack([first, second], axis=1)


def per_device(
    tokens,
    carried,
    decay_rate,
    frequency,
    log_step,
    in_map,
    out_map,
    skip_gain,
    norm_gain,
    w_in,
    w_out,
    expert_gain,
    route_ids,
    route_logit,
    w_gate,
    w_up,
    w_down,
):
    count_rows, model_width = tokens.shape
    core = lax.axis_index("tp")
    slots = CAP // lax.axis_size("tp")
    normed = normalize(tokens, norm_gain)
    drive = jnp.dot(normed, w_in, preferred_element_type=jnp.float32).astype(jnp.bfloat16)
    activated, new_carried = state_update(
        drive, carried, decay_rate, frequency, log_step, in_map, out_map, skip_gain
    )
    partial_value = jnp.dot(activated, w_out, preferred_element_type=jnp.float32).astype(
        jnp.bfloat16
    )
    summed = partial_value.astype(jnp.float32) + swapped(partial_value).astype(jnp.float32)
    mixed = (tokens.astype(jnp.float32) + summed).astype(jnp.bfloat16)
    expert_in = normalize(mixed, expert_gain)
    weights = route_weights(route_logit)
    gates = (w_gate.T, swapped(w_gate.T))
    ups = (w_up.T, swapped(w_up.T))
    downs = (w_down, swapped(w_down))
    chip = lax.axis_index("ep")
    own_z, own_y = chip // (Y_SIZE * X_SIZE), chip // X_SIZE % Y_SIZE
    expert_z, expert_y = route_ids // 2, route_ids % 2
    differ = (gray(expert_z) ^ gray(own_z), expert_y ^ (own_y >> 1))
    block = ((differ[0] & 1) * 4 + (differ[0] >> 1) * 2 + differ[1]).reshape(-1)
    expert_ids = jnp.arange(EXPERTS, dtype=jnp.int32)
    routes_flat = route_ids.reshape(-1)
    weights_flat = weights.reshape(-1)
    onehot = (routes_flat[:, None] == expert_ids[None, :]).astype(jnp.int32)
    earlier = jnp.cumsum(onehot, axis=0) - onehot
    slot_index = jnp.sum(earlier * onehot, axis=1) - core * slots
    held = (slot_index >= 0) & (slot_index < slots)
    position = jnp.where(held, block * slots + slot_index, -1)
    placement = (
        jnp.arange(EXPERTS * slots, dtype=jnp.int32)[:, None] == position[None, :]
    ).astype(jnp.float32)
    per_token = placement.reshape(EXPERTS * slots, count_rows, TOP).sum(axis=2)
    packed = jnp.dot(per_token.astype(jnp.bfloat16), expert_in, preferred_element_type=jnp.float32)
    blocks = packed.astype(jnp.bfloat16).reshape(EXPERTS, slots, model_width)
    came = [blocks[0]] + [
        over_links(blocks[index], select_links(index)) for index in range(1, EXPERTS)
    ]
    near, far = [], []
    for colour, (first, last) in enumerate(COLOURS):
        rows = jnp.concatenate(came[first:last], axis=0)
        for step in range(2):
            across = over_links(rows, spread_links(step, colour))
            rows = jnp.concatenate([rows, across], axis=0)
        near.append(rows)
        far.append(over_links(rows, spread_links(2, colour)))
    near_out = experts(near, gates, ups, downs, jnp.float32)
    far_out = experts(far, gates, ups, downs, jnp.bfloat16)
    sums = []
    for colour in range(len(COLOURS)):
        across = over_links(far_out[colour], spread_links(2, colour))
        total = near_out[colour] + across.astype(jnp.float32)
        for step in (1, 0):
            half = total.shape[0] // 2
            across = over_links(total[half:].astype(jnp.bfloat16), spread_links(step, colour))
            total = total[:half] + across.astype(jnp.float32)
        sums += list(total.astype(jnp.bfloat16).reshape(-1, slots, model_width))
    back = [sums[0]] + [
        over_links(sums[index], select_links(index)) for index in range(1, EXPERTS)
    ]
    per_expert = jnp.concatenate(back, axis=0).astype(jnp.float32)
    weighing = (
        (placement * weights_flat[None, :]).reshape(EXPERTS * slots, count_rows, TOP).sum(axis=2)
    )
    expert_sum = jnp.dot(weighing.T, per_expert, preferred_element_type=jnp.float32)
    half_width = model_width // lax.axis_size("tp")
    own_sum = lax.dynamic_slice_in_dim(expert_sum, core * half_width, half_width, 1)
    other_sum = lax.dynamic_slice_in_dim(expert_sum, (1 - core) * half_width, half_width, 1)
    own_mixed = lax.dynamic_slice_in_dim(mixed, core * half_width, half_width, 1)
    new_tokens = (own_mixed.astype(jnp.float32) + (own_sum + swapped(other_sum))).astype(
        jnp.bfloat16
    )
    return (new_tokens, new_carried)


def solution(mesh):
    return jax.shard_map(
        per_device,
        mesh=mesh,
        in_specs=(
            P("ep", None),
            P("ep", "tp", None),
            P("tp", None),
            P("tp", None),
            P("tp"),
            P("tp", None, None),
            P("tp", None, None),
            P("tp"),
            P(),
            P(None, "tp"),
            P("tp", None),
            P(),
            P("ep", None),
            P("ep", None),
            P(None, ("ep", "tp")),
            P(None, ("ep", "tp")),
            P(("ep", "tp"), None),
        ),
        out_specs=(P("ep", "tp"), P("ep", "tp", None)),
        check_vma=False,
    )
```

```python
import jax
import jax.numpy as jnp
from jax import lax
from jax.experimental import pallas as pl
from jax.experimental.pallas import tpu as pltpu
from jax.sharding import PartitionSpec as P

EXPERTS = 8
TOP = 2
CAP = 16
Y_SIZE = 4
X_SIZE = 4
SELECT = ("za", "zb", "yb")
STREAMS = (
    ((0, 5), (("ya", "xa"), ("xa", "xb"), ("xb", "ya"))),
    ((5, 8), (("xb", "xb"), ("ya", "ya"), ("xa", "xa"))),
)
OUT_CHUNK = 512


def gray(value):
    return value ^ (value >> 1)


def neighbour(chip, link):
    place = {"z": chip // (Y_SIZE * X_SIZE), "y": chip // X_SIZE % Y_SIZE, "x": chip % X_SIZE}
    axis, bit = link
    code = gray(place[axis]) ^ (1 if bit == "a" else 2)
    place[axis] = code ^ (code >> 1)
    return (place["z"] * Y_SIZE + place["y"]) * X_SIZE + place["x"]


def over_links(shard, links_of_core):
    pairs = []
    for chip in range(lax.axis_size("ep")):
        for core, links in enumerate(links_of_core):
            other = chip
            for link in links:
                other = neighbour(other, link)
            pairs.append((chip * 2 + core, other * 2 + core))
    return lax.ppermute(shard, ("ep", "tp"), pairs)


def over_select(shard, block):
    links = [link for bit, link in zip((4, 2, 1), SELECT) if block & bit]
    return over_links(shard, (links, links))


def over_spread(shard, links):
    return over_links(shard, [[link] for link in links])


def swapped(shard):
    return lax.ppermute(shard, "tp", [(0, 1), (1, 0)])


def unit_cuts(units):
    cuts = []
    for first in range(0, 2 * units, 256):
        last = min(first + 256, 2 * units)
        copies = []
        for which in range(2):
            low, high = max(first, which * units), min(last, (which + 1) * units)
            if low < high:
                copies.append((which, low - which * units, low, high - low))
        cuts.append((first, last - first, copies))
    return cuts


def expert_kernel(sizes, units, *refs):
    count = len(sizes)
    pieces, refs = refs[:count], refs[count:]
    gates, ups, downs, refs = refs[0:2], refs[2:4], refs[4:6], refs[6:]
    outs, refs = refs[:count], refs[count:]
    results, refs = refs[:count], refs[count:]
    rows, gate, up, down, hidden, row_sem, unit_sem, down_sem, out_sem = refs
    starts = [sum(sizes[:index]) for index in range(count)]
    row_copies = [
        pltpu.make_async_copy(piece, rows.at[pl.ds(start, size)], row_sem.at[index])
        for index, (piece, start, size) in enumerate(zip(pieces, starts, sizes))
    ]
    cuts = unit_cuts(units)
    unit_copies = []
    number = 0
    for _, _, copies in cuts:
        chunk = []
        for which, source, target, size in copies:
            for weights, held in ((gates, gate), (ups, up)):
                chunk.append(
                    pltpu.make_async_copy(
                        weights[which].at[pl.ds(source, size)],
                        held.at[pl.ds(target, size)],
                        unit_sem.at[number],
                    )
                )
                number += 1
        unit_copies.append(chunk)
    down_copies = [
        pltpu.make_async_copy(
            downs[which], down.at[pl.ds(which * units, units)], down_sem.at[which]
        )
        for which in range(2)
    ]
    for copy in unit_copies[0] + row_copies + unit_copies[1]:
        copy.start()
    for copy in row_copies:
        copy.wait()
    contract = (((1,), (1,)), ((), ()))
    for index, (first, size, _) in enumerate(cuts):
        for copy in unit_copies[index]:
            copy.wait()
        if index + 2 < len(cuts):
            for copy in unit_copies[index + 2]:
                copy.start()
        if index + 2 == len(cuts):
            for copy in down_copies:
                copy.start()
        span = pl.ds(first, size)
        gated = lax.dot_general(
            rows[...], gate[span, :], contract, preferred_element_type=jnp.float32
        )
        upward = lax.dot_general(
            rows[...], up[span, :], contract, preferred_element_type=jnp.float32
        )
        hidden[:, span] = (jax.nn.silu(gated) * upward).astype(hidden.dtype)
    for copy in down_copies:
        copy.wait()
    out_copies = []
    for step in range(down.shape[1] // OUT_CHUNK):
        span = pl.ds(step * OUT_CHUNK, OUT_CHUNK)
        produced = jnp.dot(hidden[...], down[:, span], preferred_element_type=jnp.float32)
        for index, (out, result) in enumerate(zip(outs, results)):
            start, size = starts[index], sizes[index]
            result[:, span] = produced[start : start + size].astype(result.dtype)
            copy = pltpu.make_async_copy(
                result.at[:, span], out.at[:, span], out_sem.at[step, index]
            )
            copy.start()
            out_copies.append(copy)
    for copy in out_copies:
        copy.wait()


def experts(pieces, gates, ups, downs, dtypes):
    sizes = [piece.shape[0] for piece in pieces]
    units, width = gates[0].shape
    count_rows = sum(sizes)
    copies = 2 * sum(len(cut[2]) for cut in unit_cuts(units))
    whole = pl.BlockSpec(memory_space=pl.ANY)
    held = pltpu.VMEM((2 * units, width), jnp.bfloat16)
    return pl.pallas_call(
        lambda *refs: expert_kernel(sizes, units, *refs),
        out_shape=[
            jax.ShapeDtypeStruct((size, width), dtype) for size, dtype in zip(sizes, dtypes)
        ],
        in_specs=[whole] * (len(pieces) + 6),
        out_specs=[whole] * len(pieces),
        scratch_shapes=[pltpu.VMEM((size, width), dtype) for size, dtype in zip(sizes, dtypes)]
        + [
            pltpu.VMEM((count_rows, width), jnp.bfloat16),
            held,
            held,
            held,
            pltpu.VMEM((count_rows, 2 * units), jnp.bfloat16),
            pltpu.SemaphoreType.DMA((len(pieces),)),
            pltpu.SemaphoreType.DMA((copies,)),
            pltpu.SemaphoreType.DMA((2,)),
            pltpu.SemaphoreType.DMA((width // OUT_CHUNK, len(pieces))),
        ],
        compiler_params=pltpu.CompilerParams(vmem_limit_bytes=40 * 1024 * 1024),
        cost_estimate=pl.CostEstimate(
            flops=12 * count_rows * units * width,
            transcendentals=2 * count_rows * units,
            bytes_accessed=12 * units * width + 4 * count_rows * width,
        ),
        name="experts",
    )(*pieces, *gates, *ups, *downs)


def normalize(rows, gain):
    wide = rows.astype(jnp.float32)
    scaled = wide * lax.rsqrt(jnp.mean(wide * wide, axis=-1, keepdims=True) + 1e-06)
    return (scaled * gain).astype(jnp.bfloat16)


def state_update(drive, carried, decay_rate, frequency, log_step, in_map, out_map, skip_gain):
    count_rows, width = drive.shape
    groups, half = decay_rate.shape
    channels = width // groups
    step_size = jnp.exp(log_step)[:, None]
    magnitude = jnp.exp(-decay_rate * step_size)
    real_decay = magnitude * jnp.cos(frequency * step_size)
    imag_decay = magnitude * jnp.sin(frequency * step_size)
    denom = decay_rate * decay_rate + frequency * frequency
    real_less = real_decay - 1.0
    real_factor = (-real_less * decay_rate + imag_decay * frequency) / denom
    imag_factor = (-imag_decay * decay_rate - real_less * frequency) / denom
    grouped_drive = drive.reshape(count_rows, groups, channels)
    projected = jnp.einsum(
        "sgh,gqh->sgq", grouped_drive, in_map, preferred_element_type=jnp.float32
    )
    real_in = projected[..., :half]
    imag_in = projected[..., half:]
    real_push = real_factor * real_in - imag_factor * imag_in
    imag_push = real_factor * imag_in + imag_factor * real_in
    real_old = carried[..., :half]
    imag_old = carried[..., half:]
    real_new = real_decay * real_old - imag_decay * imag_old + real_push
    imag_new = real_decay * imag_old + imag_decay * real_old + imag_push
    joined = jnp.concatenate([real_new, -imag_new], axis=-1)
    reading = jnp.einsum("sgq,ghq->sgh", joined, out_map.astype(jnp.float32))
    total = reading.reshape(count_rows, width) + skip_gain * drive.astype(jnp.float32)
    activated = jax.nn.gelu(total).astype(jnp.bfloat16)
    return (activated, jnp.concatenate([real_new, imag_new], axis=-1))


def route_weights(route_logit):
    first = jax.nn.sigmoid(route_logit[:, 0] - route_logit[:, 1])
    second = jax.nn.sigmoid(route_logit[:, 1] - route_logit[:, 0])
    return jnp.stack([first, second], axis=1)


def per_device(
    tokens,
    carried,
    decay_rate,
    frequency,
    log_step,
    in_map,
    out_map,
    skip_gain,
    norm_gain,
    w_in,
    w_out,
    expert_gain,
    route_ids,
    route_logit,
    w_gate,
    w_up,
    w_down,
):
    count_rows, model_width = tokens.shape
    core = lax.axis_index("tp")
    slots = CAP // lax.axis_size("tp")
    normed = normalize(tokens, norm_gain)
    drive = jnp.dot(normed, w_in, preferred_element_type=jnp.float32).astype(jnp.bfloat16)
    activated, new_carried = state_update(
        drive, carried, decay_rate, frequency, log_step, in_map, out_map, skip_gain
    )
    partial_value = jnp.dot(activated, w_out, preferred_element_type=jnp.float32).astype(
        jnp.bfloat16
    )
    summed = partial_value.astype(jnp.float32) + swapped(partial_value).astype(jnp.float32)
    mixed = (tokens.astype(jnp.float32) + summed).astype(jnp.bfloat16)
    expert_in = normalize(mixed, expert_gain)
    weights = route_weights(route_logit)
    gates = (w_gate.T, swapped(w_gate.T))
    ups = (w_up.T, swapped(w_up.T))
    downs = (w_down, swapped(w_down))
    chip = lax.axis_index("ep")
    own_z, own_y = chip // (Y_SIZE * X_SIZE), chip // X_SIZE % Y_SIZE
    expert_z, expert_y = route_ids // 2, route_ids % 2
    differ = (gray(expert_z) ^ gray(own_z), expert_y ^ (own_y >> 1))
    block = ((differ[0] & 1) * 4 + (differ[0] >> 1) * 2 + differ[1]).reshape(-1)
    expert_ids = jnp.arange(EXPERTS, dtype=jnp.int32)
    routes_flat = route_ids.reshape(-1)
    weights_flat = weights.reshape(-1)
    onehot = (routes_flat[:, None] == expert_ids[None, :]).astype(jnp.int32)
    earlier = jnp.cumsum(onehot, axis=0) - onehot
    slot_index = jnp.sum(earlier * onehot, axis=1) - core * slots
    held = (slot_index >= 0) & (slot_index < slots)
    position = jnp.where(held, block * slots + slot_index, -1)
    placement = (
        jnp.arange(EXPERTS * slots, dtype=jnp.int32)[:, None] == position[None, :]
    ).astype(jnp.float32)
    per_token = placement.reshape(EXPERTS * slots, count_rows, TOP).sum(axis=2)
    packed = jnp.dot(per_token.astype(jnp.bfloat16), expert_in, preferred_element_type=jnp.float32)
    blocks = packed.astype(jnp.bfloat16).reshape(EXPERTS, slots, model_width)
    came = [blocks[0]] + [
        over_select(blocks[index], index) for index in range(1, EXPERTS)
    ]
    sums = []
    for (first, last), links in STREAMS:
        rows = jnp.concatenate(came[first:last], axis=0)
        for step in range(2):
            rows = jnp.concatenate([rows, over_spread(rows, links[step])], axis=0)
        far = over_spread(rows, links[2])
        total, far_out = experts(
            (rows, far), gates, ups, downs, (jnp.float32, jnp.bfloat16)
        )
        total = total + over_spread(far_out, links[2]).astype(jnp.float32)
        for step in (1, 0):
            half = total.shape[0] // 2
            across = over_spread(total[half:].astype(jnp.bfloat16), links[step])
            total = total[:half] + across.astype(jnp.float32)
        sums += list(total.astype(jnp.bfloat16).reshape(-1, slots, model_width))
    back = [sums[0]] + [
        over_select(sums[index], index) for index in range(1, EXPERTS)
    ]
    per_expert = jnp.concatenate(back, axis=0).astype(jnp.float32)
    weighing = (
        (placement * weights_flat[None, :]).reshape(EXPERTS * slots, count_rows, TOP).sum(axis=2)
    )
    expert_sum = jnp.dot(weighing.T, per_expert, preferred_element_type=jnp.float32)
    half_width = model_width // lax.axis_size("tp")
    own_sum = lax.dynamic_slice_in_dim(expert_sum, core * half_width, half_width, 1)
    other_sum = lax.dynamic_slice_in_dim(expert_sum, (1 - core) * half_width, half_width, 1)
    own_mixed = lax.dynamic_slice_in_dim(mixed, core * half_width, half_width, 1)
    new_tokens = (own_mixed.astype(jnp.float32) + (own_sum + swapped(other_sum))).astype(
        jnp.bfloat16
    )
    return (new_tokens, new_carried)


def solution(mesh):
    return jax.shard_map(
        per_device,
        mesh=mesh,
        in_specs=(
            P("ep", None),
            P("ep", "tp", None),
            P("tp", None),
            P("tp", None),
            P("tp"),
            P("tp", None, None),
            P("tp", None, None),
            P("tp"),
            P(),
            P(None, "tp"),
            P("tp", None),
            P(),
            P("ep", None),
            P("ep", None),
            P(None, ("ep", "tp")),
            P(None, ("ep", "tp")),
            P(("ep", "tp"), None),
        ),
        out_specs=(P("ep", "tp"), P("ep", "tp", None)),
        check_vma=False,
    )
```

```python
import jax
import jax.numpy as jnp
from jax import lax
from jax.experimental import pallas as pl
from jax.experimental.pallas import tpu as pltpu
from jax.sharding import PartitionSpec as P

EXPERTS = 8
TOP = 2
CAP = 16
Y_SIZE = 4
X_SIZE = 4
SELECT = ("za", "zb", "yb")
SPREAD = ("ya", "xa", "xb")
COLOURS = ((0, 3), (3, 6), (6, 8))
UNIT_CHUNK = 256
OUT_CHUNK = 512


def gray(value):
    return value ^ (value >> 1)


def neighbour(chip, link):
    place = {"z": chip // (Y_SIZE * X_SIZE), "y": chip // X_SIZE % Y_SIZE, "x": chip % X_SIZE}
    axis, bit = link
    code = gray(place[axis]) ^ (1 if bit == "a" else 2)
    place[axis] = code ^ (code >> 1)
    return (place["z"] * Y_SIZE + place["y"]) * X_SIZE + place["x"]


def over_links(shard, links):
    pairs = []
    for chip in range(lax.axis_size("ep")):
        other = chip
        for link in links:
            other = neighbour(other, link)
        pairs += [(chip * 2 + core, other * 2 + core) for core in range(2)]
    return lax.ppermute(shard, ("ep", "tp"), pairs)


def select_links(block):
    return [link for bit, link in zip((4, 2, 1), SELECT) if block & bit]


def spread_links(step, colour):
    return [SPREAD[(step + colour) % 3]]


def swapped(shard):
    return lax.ppermute(shard, "tp", [(0, 1), (1, 0)])


def load_kernel(units, *refs):
    sources, helds, sem = refs[0:6], refs[-4:-1], refs[-1]
    copies = [
        pltpu.make_async_copy(
            source, helds[index // 2].at[pl.ds(index % 2 * units, units)], sem.at[index]
        )
        for index, source in enumerate(sources)
    ]
    for copy in copies:
        copy.start()
    for copy in copies:
        copy.wait()


def loaded(gates, ups, downs, after):
    units, width = gates[0].shape
    whole = pl.BlockSpec(memory_space=pl.ANY)
    return pl.pallas_call(
        lambda *refs: load_kernel(units, *refs),
        out_shape=[pltpu.VMEM((2 * units, width), jnp.bfloat16)] * 3,
        in_specs=[whole] * (6 + len(after)),
        out_specs=[pl.BlockSpec(memory_space=pltpu.VMEM)] * 3,
        scratch_shapes=[pltpu.SemaphoreType.DMA((6,))],
        compiler_params=pltpu.CompilerParams(vmem_limit_bytes=2 * 1024 * 1024),
        cost_estimate=pl.CostEstimate(
            flops=6 * units * width * 2048,
            transcendentals=0,
            bytes_accessed=12 * units * width,
        ),
        name="load",
    )(*gates, *ups, *downs, *after)


def expert_kernel(sizes, targets, *refs):
    count = len(sizes)
    pieces, (gate, up, down, out, rows, hidden, row_sem) = refs[:count], refs[count:]
    row_copies = [
        pltpu.make_async_copy(
            piece, rows.at[pl.ds(sum(sizes[:index]), sizes[index])], row_sem.at[index]
        )
        for index, piece in enumerate(pieces)
    ]
    for copy in row_copies:
        copy.start()
    for copy in row_copies:
        copy.wait()
    contract = (((1,), (1,)), ((), ()))
    units = gate.shape[0]
    for first in range(0, units, UNIT_CHUNK):
        span = pl.ds(first, min(UNIT_CHUNK, units - first))
        gated = lax.dot_general(
            rows[...], gate[span, :], contract, preferred_element_type=jnp.float32
        )
        upward = lax.dot_general(
            rows[...], up[span, :], contract, preferred_element_type=jnp.float32
        )
        hidden[:, span] = (jax.nn.silu(gated) * upward).astype(hidden.dtype)
    slots = out.shape[1]
    for step in range(down.shape[1] // OUT_CHUNK):
        span = pl.ds(step * OUT_CHUNK, OUT_CHUNK)
        produced = jnp.dot(
            hidden[...], down[:, span], preferred_element_type=jnp.float32
        ).astype(out.dtype)
        for block in range(out.shape[0]):
            out[targets[block], :, span] = produced[block * slots : (block + 1) * slots]


def experts(pieces, targets, held, slots):
    sizes = [piece.shape[0] for piece in pieces]
    units, width = held[0].shape
    count_rows = sum(sizes)
    whole = pl.BlockSpec(memory_space=pl.ANY)
    vmem = pl.BlockSpec(memory_space=pltpu.VMEM)
    return pl.pallas_call(
        lambda targets, *refs: expert_kernel(sizes, targets, *refs),
        out_shape=pltpu.VMEM((count_rows // slots, slots, width), jnp.bfloat16),
        in_specs=[pl.BlockSpec(memory_space=pltpu.SMEM)] + [whole] * len(pieces) + [vmem] * 3,
        out_specs=vmem,
        scratch_shapes=[
            pltpu.VMEM((count_rows, width), jnp.bfloat16),
            pltpu.VMEM((count_rows, units), jnp.bfloat16),
            pltpu.SemaphoreType.DMA((len(pieces),)),
        ],
        compiler_params=pltpu.CompilerParams(vmem_limit_bytes=20 * 1024 * 1024),
        cost_estimate=pl.CostEstimate(
            flops=6 * count_rows * units * width,
            transcendentals=count_rows * units,
            bytes_accessed=4 * count_rows * width,
        ),
        name="experts",
    )(targets, *pieces, *held)


def link_mask(links):
    place = {"z": 16, "y": 4, "x": 1}
    return sum(place[link[0]] * (1 if link[1] == "a" else 2) for link in links)


def block_targets():
    masks = []
    for steps in (range(4), range(4, 8)):
        for colour, (first, last) in enumerate(COLOURS):
            for crossed in steps:
                spread = [spread_links(bit, colour)[0] for bit in range(3) if crossed >> bit & 1]
                masks += [link_mask(spread + select_links(block)) for block in range(first, last)]
    chip = lax.axis_index("ep")
    own = gray(chip // 16) * 16 + gray(chip // 4 % 4) * 4 + gray(chip % 4)
    code = own ^ jnp.array(masks, jnp.int32)
    return code ^ (code >> 1 & 21)


def normalize(rows, gain):
    wide = rows.astype(jnp.float32)
    scaled = wide * lax.rsqrt(jnp.mean(wide * wide, axis=-1, keepdims=True) + 1e-06)
    return (scaled * gain).astype(jnp.bfloat16)


def state_update(drive, carried, decay_rate, frequency, log_step, in_map, out_map, skip_gain):
    count_rows, width = drive.shape
    groups, half = decay_rate.shape
    channels = width // groups
    step_size = jnp.exp(log_step)[:, None]
    magnitude = jnp.exp(-decay_rate * step_size)
    real_decay = magnitude * jnp.cos(frequency * step_size)
    imag_decay = magnitude * jnp.sin(frequency * step_size)
    denom = decay_rate * decay_rate + frequency * frequency
    real_less = real_decay - 1.0
    real_factor = (-real_less * decay_rate + imag_decay * frequency) / denom
    imag_factor = (-imag_decay * decay_rate - real_less * frequency) / denom
    grouped_drive = drive.reshape(count_rows, groups, channels)
    projected = jnp.einsum(
        "sgh,gqh->sgq", grouped_drive, in_map, preferred_element_type=jnp.float32
    )
    real_in = projected[..., :half]
    imag_in = projected[..., half:]
    real_push = real_factor * real_in - imag_factor * imag_in
    imag_push = real_factor * imag_in + imag_factor * real_in
    real_old = carried[..., :half]
    imag_old = carried[..., half:]
    real_new = real_decay * real_old - imag_decay * imag_old + real_push
    imag_new = real_decay * imag_old + imag_decay * real_old + imag_push
    joined = jnp.concatenate([real_new, -imag_new], axis=-1)
    reading = jnp.einsum("sgq,ghq->sgh", joined, out_map.astype(jnp.float32))
    total = reading.reshape(count_rows, width) + skip_gain * drive.astype(jnp.float32)
    activated = jax.nn.gelu(total).astype(jnp.bfloat16)
    return (activated, jnp.concatenate([real_new, imag_new], axis=-1))


def route_weights(route_logit):
    first = jax.nn.sigmoid(route_logit[:, 0] - route_logit[:, 1])
    second = jax.nn.sigmoid(route_logit[:, 1] - route_logit[:, 0])
    return jnp.stack([first, second], axis=1)


def per_device(
    tokens,
    carried,
    decay_rate,
    frequency,
    log_step,
    in_map,
    out_map,
    skip_gain,
    norm_gain,
    w_in,
    w_out,
    expert_gain,
    route_ids,
    route_logit,
    w_gate,
    w_up,
    w_down,
):
    count_rows, model_width = tokens.shape
    core = lax.axis_index("tp")
    slots = CAP // lax.axis_size("tp")
    normed = normalize(tokens, norm_gain)
    drive = jnp.dot(normed, w_in, preferred_element_type=jnp.float32).astype(jnp.bfloat16)
    activated, new_carried = state_update(
        drive, carried, decay_rate, frequency, log_step, in_map, out_map, skip_gain
    )
    partial_value = jnp.dot(activated, w_out, preferred_element_type=jnp.float32).astype(
        jnp.bfloat16
    )
    summed = partial_value.astype(jnp.float32) + swapped(partial_value).astype(jnp.float32)
    mixed = (tokens.astype(jnp.float32) + summed).astype(jnp.bfloat16)
    expert_in = normalize(mixed, expert_gain)
    weights = route_weights(route_logit)
    gates = (w_gate.T, swapped(w_gate.T))
    ups = (w_up.T, swapped(w_up.T))
    downs = (w_down, swapped(w_down))
    chip = lax.axis_index("ep")
    own_z, own_y = chip // (Y_SIZE * X_SIZE), chip // X_SIZE % Y_SIZE
    expert_ids = jnp.arange(EXPERTS, dtype=jnp.int32)
    differ_z, differ_y = gray(expert_ids // 2) ^ gray(own_z), expert_ids % 2 ^ (own_y >> 1)
    block_of = (differ_z & 1) * 4 + (differ_z >> 1) * 2 + differ_y
    routes_flat = route_ids.reshape(-1)
    weights_flat = weights.reshape(-1)
    onehot = (routes_flat[:, None] == expert_ids[None, :]).astype(jnp.int32)
    earlier = jnp.cumsum(onehot, axis=0) - onehot
    slot_index = jnp.sum(earlier * onehot, axis=1) - core * slots
    block = jnp.sum(block_of[None, :] * onehot, axis=1)
    held = (slot_index >= 0) & (slot_index < slots)
    row_ids = jnp.arange(EXPERTS * slots, dtype=jnp.int32)[:, None]
    sent_to = jnp.where(held, block * slots + slot_index, -1)
    position = jnp.where(held, routes_flat * slots + slot_index, -1)
    sending = (row_ids == sent_to[None, :]).astype(jnp.float32)
    placement = (row_ids == position[None, :]).astype(jnp.float32)
    per_token = sending.reshape(EXPERTS * slots, count_rows, TOP).sum(axis=2)
    packed = jnp.dot(per_token.astype(jnp.bfloat16), expert_in, preferred_element_type=jnp.float32)
    blocks = packed.astype(jnp.bfloat16).reshape(EXPERTS, slots, model_width)
    came = [blocks[0]] + [
        over_links(blocks[index], select_links(index)) for index in range(1, EXPERTS)
    ]
    near, far = [], []
    for colour, (first, last) in enumerate(COLOURS):
        rows = jnp.concatenate(came[first:last], axis=0)
        for step in range(2):
            across = over_links(rows, spread_links(step, colour))
            rows = jnp.concatenate([rows, across], axis=0)
        near.append(rows)
        far.append(over_links(rows, spread_links(2, colour)))
    held_units = loaded(gates, ups, downs, near)
    produced = experts(near + far, block_targets(), held_units, slots)
    returned = lax.all_to_all(produced, "ep", split_axis=0, concat_axis=0, tiled=True)
    per_expert = returned.reshape(EXPERTS, -1, slots, model_width).astype(jnp.float32).sum(axis=1)
    per_expert = per_expert.reshape(EXPERTS * slots, model_width)
    weighing = (
        (placement * weights_flat[None, :]).reshape(EXPERTS * slots, count_rows, TOP).sum(axis=2)
    )
    expert_sum = jnp.dot(weighing.T, per_expert, preferred_element_type=jnp.float32)
    half_width = model_width // lax.axis_size("tp")
    own_sum = lax.dynamic_slice_in_dim(expert_sum, core * half_width, half_width, 1)
    other_sum = lax.dynamic_slice_in_dim(expert_sum, (1 - core) * half_width, half_width, 1)
    own_mixed = lax.dynamic_slice_in_dim(mixed, core * half_width, half_width, 1)
    new_tokens = (own_mixed.astype(jnp.float32) + (own_sum + swapped(other_sum))).astype(
        jnp.bfloat16
    )
    return (new_tokens, new_carried)


def solution(mesh):
    return jax.shard_map(
        per_device,
        mesh=mesh,
        in_specs=(
            P("ep", None),
            P("ep", "tp", None),
            P("tp", None),
            P("tp", None),
            P("tp"),
            P("tp", None, None),
            P("tp", None, None),
            P("tp"),
            P(),
            P(None, "tp"),
            P("tp", None),
            P(),
            P("ep", None),
            P("ep", None),
            P(None, ("ep", "tp")),
            P(None, ("ep", "tp")),
            P(("ep", "tp"), None),
        ),
        out_specs=(P("ep", "tp"), P("ep", "tp", None)),
        check_vma=False,
    )
```

```python
import jax
import jax.numpy as jnp
from jax import lax
from jax.experimental import pallas as pl
from jax.experimental.pallas import tpu as pltpu
from jax.sharding import PartitionSpec as P

EXPERTS = 8
TOP = 2
CAP = 16
Y_SIZE = 4
X_SIZE = 4
SELECT = ("za", "zb", "yb")
SPREAD = ("ya", "xa", "xb")
COLOURS = ((0, 3), (3, 6), (6, 8))
UNIT_CHUNK = 256
OUT_CHUNK = 512
COPY_GROUPS = 2


def gray(value):
    return value ^ (value >> 1)


def neighbour(chip, link):
    place = {"z": chip // (Y_SIZE * X_SIZE), "y": chip // X_SIZE % Y_SIZE, "x": chip % X_SIZE}
    axis, bit = link
    code = gray(place[axis]) ^ (1 if bit == "a" else 2)
    place[axis] = code ^ (code >> 1)
    return (place["z"] * Y_SIZE + place["y"]) * X_SIZE + place["x"]


def over_links(shard, links):
    pairs = []
    for chip in range(lax.axis_size("ep")):
        other = chip
        for link in links:
            other = neighbour(other, link)
        pairs += [(chip * 2 + core, other * 2 + core) for core in range(2)]
    return lax.ppermute(shard, ("ep", "tp"), pairs)


def select_links(block):
    return [link for bit, link in zip((4, 2, 1), SELECT) if block & bit]


def spread_links(step, colour):
    return [SPREAD[(step + colour) % 3]]


def swapped(shard):
    return lax.ppermute(shard, "tp", [(0, 1), (1, 0)])


def load_kernel(units, *refs):
    sources, helds, sem = refs[0:6], refs[-4:-1], refs[-1]
    copies = [
        pltpu.make_async_copy(
            source, helds[index // 2].at[pl.ds(index % 2 * units, units)], sem.at[index]
        )
        for index, source in enumerate(sources)
    ]
    for copy in copies:
        copy.start()
    for copy in copies:
        copy.wait()


def loaded(gates, ups, downs, after):
    units, width = gates[0].shape
    whole = pl.BlockSpec(memory_space=pl.ANY)
    return pl.pallas_call(
        lambda *refs: load_kernel(units, *refs),
        out_shape=[pltpu.VMEM((2 * units, width), jnp.bfloat16)] * 3,
        in_specs=[whole] * (6 + len(after)),
        out_specs=[pl.BlockSpec(memory_space=pltpu.VMEM)] * 3,
        scratch_shapes=[pltpu.SemaphoreType.DMA((6,))],
        compiler_params=pltpu.CompilerParams(vmem_limit_bytes=2 * 1024 * 1024),
        cost_estimate=pl.CostEstimate(
            flops=6 * units * width * 2048,
            transcendentals=0,
            bytes_accessed=12 * units * width,
        ),
        name="load",
    )(*gates, *ups, *downs, *after)


def expert_kernel(sizes, targets, *refs):
    count = len(sizes)
    pieces, (gate, up, down) = refs[:count], refs[count : count + 3]
    out, rows, hidden, result, row_sem, out_sem = refs[-6:]
    row_copies = [
        pltpu.make_async_copy(
            piece, rows.at[pl.ds(sum(sizes[:index]), sizes[index])], row_sem.at[index]
        )
        for index, piece in enumerate(pieces)
    ]
    for copy in row_copies:
        copy.start()
    for copy in row_copies:
        copy.wait()
    contract = (((1,), (1,)), ((), ()))
    units = gate.shape[0]
    for first in range(0, units, UNIT_CHUNK):
        span = pl.ds(first, min(UNIT_CHUNK, units - first))
        gated = lax.dot_general(
            rows[...], gate[span, :], contract, preferred_element_type=jnp.float32
        )
        upward = lax.dot_general(
            rows[...], up[span, :], contract, preferred_element_type=jnp.float32
        )
        hidden[:, span] = (jax.nn.silu(gated) * upward).astype(hidden.dtype)
    slots, width = out.shape[1:]
    out_copies = []
    for first in range(0, width, OUT_CHUNK):
        span = pl.ds(first, OUT_CHUNK)
        result[:, span] = jnp.dot(
            hidden[...], down[:, span], preferred_element_type=jnp.float32
        ).astype(result.dtype)
        done = first + OUT_CHUNK
        if done % (width // COPY_GROUPS):
            continue
        group = done * COPY_GROUPS // width - 1
        columns = pl.ds(group * (width // COPY_GROUPS), width // COPY_GROUPS)
        for block in range(sum(sizes) // slots):
            copy = pltpu.make_async_copy(
                result.at[pl.ds(block * slots, slots), columns],
                out.at[targets[block], :, columns],
                out_sem.at[group, block],
            )
            copy.start()
            out_copies.append(copy)
    for copy in out_copies:
        copy.wait()


def experts(pieces, targets, held, slots, earlier=()):
    sizes = [piece.shape[0] for piece in pieces]
    units, width = held[0].shape
    count_rows = sum(sizes)
    whole = pl.BlockSpec(memory_space=pl.ANY)
    vmem = pl.BlockSpec(memory_space=pltpu.VMEM)
    first = 1 + len(pieces) + len(held)
    return pl.pallas_call(
        lambda targets, *refs: expert_kernel(sizes, targets, *refs),
        out_shape=jax.ShapeDtypeStruct((lax.axis_size("ep"), slots, width), jnp.bfloat16),
        in_specs=[pl.BlockSpec(memory_space=pltpu.SMEM)]
        + [whole] * len(pieces)
        + [vmem] * len(held)
        + [whole] * len(earlier),
        out_specs=whole,
        input_output_aliases={first: 0} if earlier else {},
        scratch_shapes=[
            pltpu.VMEM((count_rows, width), jnp.bfloat16),
            pltpu.VMEM((count_rows, units), jnp.bfloat16),
            pltpu.VMEM((count_rows, width), jnp.bfloat16),
            pltpu.SemaphoreType.DMA((len(pieces),)),
            pltpu.SemaphoreType.DMA((COPY_GROUPS, count_rows // slots)),
        ],
        compiler_params=pltpu.CompilerParams(vmem_limit_bytes=16 * 1024 * 1024),
        cost_estimate=pl.CostEstimate(
            flops=6 * count_rows * units * width,
            transcendentals=count_rows * units,
            bytes_accessed=4 * count_rows * width,
        ),
        name="experts",
    )(targets, *pieces, *held, *earlier)


def link_mask(links):
    place = {"z": 16, "y": 4, "x": 1}
    return sum(place[link[0]] * (1 if link[1] == "a" else 2) for link in links)


def block_targets():
    masks = []
    for steps in (range(4), range(4, 8)):
        for colour, (first, last) in enumerate(COLOURS):
            for crossed in steps:
                spread = [spread_links(bit, colour)[0] for bit in range(3) if crossed >> bit & 1]
                masks += [link_mask(spread + select_links(block)) for block in range(first, last)]
    chip = lax.axis_index("ep")
    own = gray(chip // 16) * 16 + gray(chip // 4 % 4) * 4 + gray(chip % 4)
    code = own ^ jnp.array(masks, jnp.int32)
    return code ^ (code >> 1 & 21)


def normalize(rows, gain):
    wide = rows.astype(jnp.float32)
    scaled = wide * lax.rsqrt(jnp.mean(wide * wide, axis=-1, keepdims=True) + 1e-06)
    return (scaled * gain).astype(jnp.bfloat16)


def state_update(drive, carried, decay_rate, frequency, log_step, in_map, out_map, skip_gain):
    count_rows, width = drive.shape
    groups, half = decay_rate.shape
    channels = width // groups
    step_size = jnp.exp(log_step)[:, None]
    magnitude = jnp.exp(-decay_rate * step_size)
    real_decay = magnitude * jnp.cos(frequency * step_size)
    imag_decay = magnitude * jnp.sin(frequency * step_size)
    denom = decay_rate * decay_rate + frequency * frequency
    real_less = real_decay - 1.0
    real_factor = (-real_less * decay_rate + imag_decay * frequency) / denom
    imag_factor = (-imag_decay * decay_rate - real_less * frequency) / denom
    grouped_drive = drive.reshape(count_rows, groups, channels)
    projected = jnp.einsum(
        "sgh,gqh->sgq", grouped_drive, in_map, preferred_element_type=jnp.float32
    )
    real_in = projected[..., :half]
    imag_in = projected[..., half:]
    real_push = real_factor * real_in - imag_factor * imag_in
    imag_push = real_factor * imag_in + imag_factor * real_in
    real_old = carried[..., :half]
    imag_old = carried[..., half:]
    real_new = real_decay * real_old - imag_decay * imag_old + real_push
    imag_new = real_decay * imag_old + imag_decay * real_old + imag_push
    joined = jnp.concatenate([real_new, -imag_new], axis=-1)
    reading = jnp.einsum("sgq,ghq->sgh", joined, out_map.astype(jnp.float32))
    total = reading.reshape(count_rows, width) + skip_gain * drive.astype(jnp.float32)
    activated = jax.nn.gelu(total).astype(jnp.bfloat16)
    return (activated, jnp.concatenate([real_new, imag_new], axis=-1))


def route_weights(route_logit):
    first = jax.nn.sigmoid(route_logit[:, 0] - route_logit[:, 1])
    second = jax.nn.sigmoid(route_logit[:, 1] - route_logit[:, 0])
    return jnp.stack([first, second], axis=1)


def per_device(
    tokens,
    carried,
    decay_rate,
    frequency,
    log_step,
    in_map,
    out_map,
    skip_gain,
    norm_gain,
    w_in,
    w_out,
    expert_gain,
    route_ids,
    route_logit,
    w_gate,
    w_up,
    w_down,
):
    count_rows, model_width = tokens.shape
    core = lax.axis_index("tp")
    slots = CAP // lax.axis_size("tp")
    normed = normalize(tokens, norm_gain)
    drive = jnp.dot(normed, w_in, preferred_element_type=jnp.float32).astype(jnp.bfloat16)
    activated, new_carried = state_update(
        drive, carried, decay_rate, frequency, log_step, in_map, out_map, skip_gain
    )
    partial_value = jnp.dot(activated, w_out, preferred_element_type=jnp.float32).astype(
        jnp.bfloat16
    )
    summed = partial_value.astype(jnp.float32) + swapped(partial_value).astype(jnp.float32)
    mixed = (tokens.astype(jnp.float32) + summed).astype(jnp.bfloat16)
    expert_in = normalize(mixed, expert_gain)
    weights = route_weights(route_logit)
    gates = (w_gate.T, swapped(w_gate.T))
    ups = (w_up.T, swapped(w_up.T))
    downs = (w_down, swapped(w_down))
    chip = lax.axis_index("ep")
    own_z, own_y = chip // (Y_SIZE * X_SIZE), chip // X_SIZE % Y_SIZE
    expert_ids = jnp.arange(EXPERTS, dtype=jnp.int32)
    differ_z, differ_y = gray(expert_ids // 2) ^ gray(own_z), expert_ids % 2 ^ (own_y >> 1)
    block_of = (differ_z & 1) * 4 + (differ_z >> 1) * 2 + differ_y
    routes_flat = route_ids.reshape(-1)
    weights_flat = weights.reshape(-1)
    onehot = (routes_flat[:, None] == expert_ids[None, :]).astype(jnp.int32)
    earlier = jnp.cumsum(onehot, axis=0) - onehot
    slot_index = jnp.sum(earlier * onehot, axis=1) - core * slots
    block = jnp.sum(block_of[None, :] * onehot, axis=1)
    held = (slot_index >= 0) & (slot_index < slots)
    row_ids = jnp.arange(EXPERTS * slots, dtype=jnp.int32)[:, None]
    sent_to = jnp.where(held, block * slots + slot_index, -1)
    position = jnp.where(held, routes_flat * slots + slot_index, -1)
    sending = (row_ids == sent_to[None, :]).astype(jnp.float32)
    placement = (row_ids == position[None, :]).astype(jnp.float32)
    per_token = sending.reshape(EXPERTS * slots, count_rows, TOP).sum(axis=2)
    packed = jnp.dot(per_token.astype(jnp.bfloat16), expert_in, preferred_element_type=jnp.float32)
    blocks = packed.astype(jnp.bfloat16).reshape(EXPERTS, slots, model_width)
    came = [blocks[0]] + [
        over_links(blocks[index], select_links(index)) for index in range(1, EXPERTS)
    ]
    near, far = [], []
    for colour, (first, last) in enumerate(COLOURS):
        rows = jnp.concatenate(came[first:last], axis=0)
        for step in range(2):
            across = over_links(rows, spread_links(step, colour))
            rows = jnp.concatenate([rows, across], axis=0)
        near.append(rows)
        far.append(over_links(rows, spread_links(2, colour)))
    held_units = loaded(gates, ups, downs, near)
    targets = block_targets()
    half = targets.shape[0] // 2
    produced = experts(near, targets[:half], held_units, slots)
    produced = experts(far, targets[half:], held_units, slots, (produced,))
    returned = lax.all_to_all(produced, "ep", split_axis=0, concat_axis=0, tiled=True)
    returned, new_carried = lax.optimization_barrier((returned, new_carried))
    per_expert = returned.reshape(EXPERTS, -1, slots, model_width).astype(jnp.float32).sum(axis=1)
    per_expert = per_expert.reshape(EXPERTS * slots, model_width)
    weighing = (
        (placement * weights_flat[None, :]).reshape(EXPERTS * slots, count_rows, TOP).sum(axis=2)
    )
    expert_sum = jnp.dot(weighing.T, per_expert, preferred_element_type=jnp.float32)
    half_width = model_width // lax.axis_size("tp")
    own_sum = lax.dynamic_slice_in_dim(expert_sum, core * half_width, half_width, 1)
    other_sum = lax.dynamic_slice_in_dim(expert_sum, (1 - core) * half_width, half_width, 1)
    own_mixed = lax.dynamic_slice_in_dim(mixed, core * half_width, half_width, 1)
    new_tokens = (own_mixed.astype(jnp.float32) + (own_sum + swapped(other_sum))).astype(
        jnp.bfloat16
    )
    return (new_tokens, new_carried)


def solution(mesh):
    return jax.shard_map(
        per_device,
        mesh=mesh,
        in_specs=(
            P("ep", None),
            P("ep", "tp", None),
            P("tp", None),
            P("tp", None),
            P("tp"),
            P("tp", None, None),
            P("tp", None, None),
            P("tp"),
            P(),
            P(None, "tp"),
            P("tp", None),
            P(),
            P("ep", None),
            P("ep", None),
            P(None, ("ep", "tp")),
            P(None, ("ep", "tp")),
            P(("ep", "tp"), None),
        ),
        out_specs=(P("ep", "tp"), P("ep", "tp", None)),
        check_vma=False,
    )
```

```python
import jax
import jax.numpy as jnp
from jax import lax
from jax.experimental import pallas as pl
from jax.experimental.layout import Layout, with_layout_constraint
from jax.experimental.pallas import tpu as pltpu
from jax.sharding import PartitionSpec as P

EXPERTS = 8
TOP = 2
CAP = 16
Y_SIZE = 4
X_SIZE = 4
SELECT = ("za", "zb", "yb")
SPREAD = ("ya", "xa", "xb")
COLOURS = ((0, 3), (3, 6), (6, 8))
UNIT_CHUNK = 256
OUT_CHUNK = 512
COPY_GROUPS = 2


def gray(value):
    return value ^ (value >> 1)


def neighbour(chip, link):
    place = {"z": chip // (Y_SIZE * X_SIZE), "y": chip // X_SIZE % Y_SIZE, "x": chip % X_SIZE}
    axis, bit = link
    code = gray(place[axis]) ^ (1 if bit == "a" else 2)
    place[axis] = code ^ (code >> 1)
    return (place["z"] * Y_SIZE + place["y"]) * X_SIZE + place["x"]


def over_links(shard, links):
    pairs = []
    for chip in range(lax.axis_size("ep")):
        other = chip
        for link in links:
            other = neighbour(other, link)
        pairs += [(chip * 2 + core, other * 2 + core) for core in range(2)]
    return lax.ppermute(shard, ("ep", "tp"), pairs)


def select_links(block):
    return [link for bit, link in zip((4, 2, 1), SELECT) if block & bit]


def spread_links(step, colour):
    return [SPREAD[(step + colour) % 3]]


def swapped(shard):
    return lax.ppermute(shard, "tp", [(0, 1), (1, 0)])


def load_kernel(units, *refs):
    sources, helds, sem = refs[0:6], refs[-4:-1], refs[-1]
    copies = [
        pltpu.make_async_copy(
            source, helds[index // 2].at[pl.ds(index % 2 * units, units)], sem.at[index]
        )
        for index, source in enumerate(sources)
    ]
    for copy in copies:
        copy.start()
    for copy in copies:
        copy.wait()


def loaded(gates, ups, downs, after):
    units, width = gates[0].shape
    whole = pl.BlockSpec(memory_space=pl.ANY)
    return pl.pallas_call(
        lambda *refs: load_kernel(units, *refs),
        out_shape=[pltpu.VMEM((2 * units, width), jnp.bfloat16)] * 3,
        in_specs=[whole] * (6 + len(after)),
        out_specs=[pl.BlockSpec(memory_space=pltpu.VMEM)] * 3,
        scratch_shapes=[pltpu.SemaphoreType.DMA((6,))],
        compiler_params=pltpu.CompilerParams(vmem_limit_bytes=2 * 1024 * 1024),
        cost_estimate=pl.CostEstimate(
            flops=6 * units * width * 2048,
            transcendentals=0,
            bytes_accessed=12 * units * width,
        ),
        name="load",
    )(*gates, *ups, *downs, *after)


def expert_kernel(sizes, targets, *refs):
    count = len(sizes)
    pieces, (gate, up, down) = refs[:count], refs[count : count + 3]
    out, rows, hidden, result, out_sem = refs[-5:]
    for index, piece in enumerate(pieces):
        rows[pl.ds(sum(sizes[:index]), sizes[index]), :] = piece[...]
    contract = (((1,), (1,)), ((), ()))
    units = gate.shape[0]
    for first in range(0, units, UNIT_CHUNK):
        span = pl.ds(first, min(UNIT_CHUNK, units - first))
        gated = lax.dot_general(
            rows[...], gate[span, :], contract, preferred_element_type=jnp.float32
        )
        upward = lax.dot_general(
            rows[...], up[span, :], contract, preferred_element_type=jnp.float32
        )
        hidden[:, span] = (jax.nn.silu(gated) * upward).astype(hidden.dtype)
    slots, width = out.shape[1:]
    out_copies = []
    for first in range(0, width, OUT_CHUNK):
        span = pl.ds(first, OUT_CHUNK)
        result[:, span] = jnp.dot(
            hidden[...], down[:, span], preferred_element_type=jnp.float32
        ).astype(result.dtype)
        done = first + OUT_CHUNK
        if done % (width // COPY_GROUPS):
            continue
        group = done * COPY_GROUPS // width - 1
        columns = pl.ds(group * (width // COPY_GROUPS), width // COPY_GROUPS)
        for block in range(sum(sizes) // slots):
            copy = pltpu.make_async_copy(
                result.at[pl.ds(block * slots, slots), columns],
                out.at[targets[block], :, columns],
                out_sem.at[group, block],
            )
            copy.start()
            out_copies.append(copy)
    for copy in out_copies:
        copy.wait()


def experts(pieces, targets, held, slots, earlier=()):
    sizes = [piece.shape[0] for piece in pieces]
    units, width = held[0].shape
    count_rows = sum(sizes)
    whole = pl.BlockSpec(memory_space=pl.ANY)
    vmem = pl.BlockSpec(memory_space=pltpu.VMEM)
    first = 1 + len(pieces) + len(held)
    return pl.pallas_call(
        lambda targets, *refs: expert_kernel(sizes, targets, *refs),
        out_shape=jax.ShapeDtypeStruct((lax.axis_size("ep"), slots, width), jnp.bfloat16),
        in_specs=[pl.BlockSpec(memory_space=pltpu.SMEM)]
        + [vmem] * (len(pieces) + len(held))
        + [whole] * len(earlier),
        out_specs=whole,
        input_output_aliases={first: 0} if earlier else {},
        scratch_shapes=[
            pltpu.VMEM((count_rows, width), jnp.bfloat16),
            pltpu.VMEM((count_rows, units), jnp.bfloat16),
            pltpu.VMEM((count_rows, width), jnp.bfloat16),
            pltpu.SemaphoreType.DMA((COPY_GROUPS, count_rows // slots)),
        ],
        compiler_params=pltpu.CompilerParams(vmem_limit_bytes=16 * 1024 * 1024),
        cost_estimate=pl.CostEstimate(
            flops=6 * count_rows * units * width,
            transcendentals=count_rows * units,
            bytes_accessed=4 * count_rows * width,
        ),
        name="experts",
    )(targets, *pieces, *held, *earlier)


def link_mask(links):
    place = {"z": 16, "y": 4, "x": 1}
    return sum(place[link[0]] * (1 if link[1] == "a" else 2) for link in links)


def block_targets():
    masks = []
    for steps in (range(4), range(4, 8)):
        for colour, (first, last) in enumerate(COLOURS):
            for crossed in steps:
                spread = [spread_links(bit, colour)[0] for bit in range(3) if crossed >> bit & 1]
                masks += [link_mask(spread + select_links(block)) for block in range(first, last)]
    chip = lax.axis_index("ep")
    own = gray(chip // 16) * 16 + gray(chip // 4 % 4) * 4 + gray(chip % 4)
    code = own ^ jnp.array(masks, jnp.int32)
    return code ^ (code >> 1 & 21)


def normalize(rows, gain):
    wide = rows.astype(jnp.float32)
    scaled = wide * lax.rsqrt(jnp.mean(wide * wide, axis=-1, keepdims=True) + 1e-06)
    return (scaled * gain).astype(jnp.bfloat16)


def state_update(drive, carried, decay_rate, frequency, log_step, in_map, out_map, skip_gain):
    count_rows, width = drive.shape
    groups, half = decay_rate.shape
    channels = width // groups
    step_size = jnp.exp(log_step)[:, None]
    magnitude = jnp.exp(-decay_rate * step_size)
    real_decay = magnitude * jnp.cos(frequency * step_size)
    imag_decay = magnitude * jnp.sin(frequency * step_size)
    denom = decay_rate * decay_rate + frequency * frequency
    real_less = real_decay - 1.0
    real_factor = (-real_less * decay_rate + imag_decay * frequency) / denom
    imag_factor = (-imag_decay * decay_rate - real_less * frequency) / denom
    grouped_drive = drive.reshape(count_rows, groups, channels)
    projected = jnp.einsum(
        "sgh,gqh->sgq", grouped_drive, in_map, preferred_element_type=jnp.float32
    )
    real_in = projected[..., :half]
    imag_in = projected[..., half:]
    real_push = real_factor * real_in - imag_factor * imag_in
    imag_push = real_factor * imag_in + imag_factor * real_in
    real_old = carried[..., :half]
    imag_old = carried[..., half:]
    real_new = real_decay * real_old - imag_decay * imag_old + real_push
    imag_new = real_decay * imag_old + imag_decay * real_old + imag_push
    joined = jnp.concatenate([real_new, -imag_new], axis=-1)
    reading = jnp.einsum("sgq,ghq->sgh", joined, out_map.astype(jnp.float32))
    total = reading.reshape(count_rows, width) + skip_gain * drive.astype(jnp.float32)
    activated = jax.nn.gelu(total).astype(jnp.bfloat16)
    return (activated, jnp.concatenate([real_new, imag_new], axis=-1))


def route_weights(route_logit):
    first = jax.nn.sigmoid(route_logit[:, 0] - route_logit[:, 1])
    second = jax.nn.sigmoid(route_logit[:, 1] - route_logit[:, 0])
    return jnp.stack([first, second], axis=1)


def per_device(
    tokens,
    carried,
    decay_rate,
    frequency,
    log_step,
    in_map,
    out_map,
    skip_gain,
    norm_gain,
    w_in,
    w_out,
    expert_gain,
    route_ids,
    route_logit,
    w_gate,
    w_up,
    w_down,
):
    count_rows, model_width = tokens.shape
    core = lax.axis_index("tp")
    slots = CAP // lax.axis_size("tp")
    normed = normalize(tokens, norm_gain)
    drive = jnp.dot(normed, w_in, preferred_element_type=jnp.float32).astype(jnp.bfloat16)
    activated, new_carried = state_update(
        drive, carried, decay_rate, frequency, log_step, in_map, out_map, skip_gain
    )
    partial_value = jnp.dot(activated, w_out, preferred_element_type=jnp.float32).astype(
        jnp.bfloat16
    )
    summed = partial_value.astype(jnp.float32) + swapped(partial_value).astype(jnp.float32)
    mixed = (tokens.astype(jnp.float32) + summed).astype(jnp.bfloat16)
    expert_in = normalize(mixed, expert_gain)
    weights = route_weights(route_logit)
    gates = (w_gate.T, swapped(w_gate.T))
    ups = (w_up.T, swapped(w_up.T))
    downs = (w_down, swapped(w_down))
    chip = lax.axis_index("ep")
    own_z, own_y = chip // (Y_SIZE * X_SIZE), chip // X_SIZE % Y_SIZE
    expert_ids = jnp.arange(EXPERTS, dtype=jnp.int32)
    differ_z, differ_y = gray(expert_ids // 2) ^ gray(own_z), expert_ids % 2 ^ (own_y >> 1)
    block_of = (differ_z & 1) * 4 + (differ_z >> 1) * 2 + differ_y
    routes_flat = route_ids.reshape(-1)
    weights_flat = weights.reshape(-1)
    onehot = (routes_flat[:, None] == expert_ids[None, :]).astype(jnp.int32)
    earlier = jnp.cumsum(onehot, axis=0) - onehot
    slot_index = jnp.sum(earlier * onehot, axis=1) - core * slots
    block = jnp.sum(block_of[None, :] * onehot, axis=1)
    held = (slot_index >= 0) & (slot_index < slots)
    row_ids = jnp.arange(EXPERTS * slots, dtype=jnp.int32)[:, None]
    sent_to = jnp.where(held, block * slots + slot_index, -1)
    position = jnp.where(held, routes_flat * slots + slot_index, -1)
    sending = (row_ids == sent_to[None, :]).astype(jnp.float32)
    placement = (row_ids == position[None, :]).astype(jnp.float32)
    per_token = sending.reshape(EXPERTS * slots, count_rows, TOP).sum(axis=2)
    packed = jnp.dot(per_token.astype(jnp.bfloat16), expert_in, preferred_element_type=jnp.float32)
    blocks = packed.astype(jnp.bfloat16).reshape(EXPERTS, slots, model_width)
    came = [blocks[0]] + [
        over_links(blocks[index], select_links(index)) for index in range(1, EXPERTS)
    ]
    near = []
    for colour, (first, last) in enumerate(COLOURS):
        rows = jnp.concatenate(came[first:last], axis=0)
        for step in range(2):
            across = over_links(rows, spread_links(step, colour))
            rows = jnp.concatenate([rows, across], axis=0)
        near.append(rows)
    held_units = loaded(gates, ups, downs, near[-1:])
    far = []
    for colour, rows in enumerate(near):
        far.append(over_links(rows, spread_links(2, colour)))
    targets = block_targets()
    half = targets.shape[0] // 2
    produced = experts(near, targets[:half], held_units, slots)
    produced = experts(far, targets[half:], held_units, slots, (produced,))
    produced, weights_flat, placement = lax.optimization_barrier(
        (produced, weights_flat, placement)
    )
    returned = lax.all_to_all(produced, "ep", split_axis=0, concat_axis=0, tiled=True)
    new_carried = with_layout_constraint(new_carried, Layout(major_to_minor=(0, 1, 2)))
    returned, new_carried = lax.optimization_barrier((returned, new_carried))
    per_expert = returned.reshape(EXPERTS, -1, slots, model_width).astype(jnp.float32).sum(axis=1)
    per_expert = per_expert.reshape(EXPERTS * slots, model_width)
    weighing = (
        (placement * weights_flat[None, :]).reshape(EXPERTS * slots, count_rows, TOP).sum(axis=2)
    )
    expert_sum = jnp.dot(weighing.T, per_expert, preferred_element_type=jnp.float32)
    half_width = model_width // lax.axis_size("tp")
    own_sum = lax.dynamic_slice_in_dim(expert_sum, core * half_width, half_width, 1)
    other_sum = lax.dynamic_slice_in_dim(expert_sum, (1 - core) * half_width, half_width, 1)
    own_mixed = lax.dynamic_slice_in_dim(mixed, core * half_width, half_width, 1)
    new_tokens = (own_mixed.astype(jnp.float32) + (own_sum + swapped(other_sum))).astype(
        jnp.bfloat16
    )
    return (new_tokens, new_carried)


def solution(mesh):
    return jax.shard_map(
        per_device,
        mesh=mesh,
        in_specs=(
            P("ep", None),
            P("ep", "tp", None),
            P("tp", None),
            P("tp", None),
            P("tp"),
            P("tp", None, None),
            P("tp", None, None),
            P("tp"),
            P(),
            P(None, "tp"),
            P("tp", None),
            P(),
            P("ep", None),
            P("ep", None),
            P(None, ("ep", "tp")),
            P(None, ("ep", "tp")),
            P(("ep", "tp"), None),
        ),
        out_specs=(P("ep", "tp"), P("ep", "tp", None)),
        check_vma=False,
    )
```

```python
import jax
import jax.numpy as jnp
from jax import lax
from jax.experimental import pallas as pl
from jax.experimental.layout import Layout, with_layout_constraint
from jax.experimental.pallas import tpu as pltpu
from jax.sharding import PartitionSpec as P

EXPERTS = 8
TOP = 2
CAP = 16
Y_SIZE = 4
X_SIZE = 4
SELECT = ("za", "zb", "yb")
SPREAD = ("ya", "xa", "xb")
COLOURS = ((0, 3), (3, 6), (6, 8))
UNIT_CHUNK = 256
OUT_CHUNK = 512
COPY_GROUPS = 2


def gray(value):
    return value ^ (value >> 1)


def neighbour(chip, link):
    place = {"z": chip // (Y_SIZE * X_SIZE), "y": chip // X_SIZE % Y_SIZE, "x": chip % X_SIZE}
    axis, bit = link
    code = gray(place[axis]) ^ (1 if bit == "a" else 2)
    place[axis] = code ^ (code >> 1)
    return (place["z"] * Y_SIZE + place["y"]) * X_SIZE + place["x"]


def over_links(shard, links):
    pairs = []
    for chip in range(lax.axis_size("ep")):
        other = chip
        for link in links:
            other = neighbour(other, link)
        pairs += [(chip * 2 + core, other * 2 + core) for core in range(2)]
    return lax.ppermute(shard, ("ep", "tp"), pairs)


def select_links(block):
    return [link for bit, link in zip((4, 2, 1), SELECT) if block & bit]


def spread_links(step, colour):
    return [SPREAD[(step + colour) % 3]]


def swapped(shard):
    return lax.ppermute(shard, "tp", [(0, 1), (1, 0)])


def load_kernel(units, *refs):
    sources, helds, sem = refs[0:6], refs[-4:-1], refs[-1]
    copies = [
        pltpu.make_async_copy(
            source, helds[index // 2].at[pl.ds(index % 2 * units, units)], sem.at[index]
        )
        for index, source in enumerate(sources)
    ]
    for copy in copies:
        copy.start()
    for copy in copies:
        copy.wait()


def loaded(gates, ups, downs, after):
    units, width = gates[0].shape
    whole = pl.BlockSpec(memory_space=pl.ANY)
    return pl.pallas_call(
        lambda *refs: load_kernel(units, *refs),
        out_shape=[pltpu.VMEM((2 * units, width), jnp.bfloat16)] * 3,
        in_specs=[whole] * (6 + len(after)),
        out_specs=[pl.BlockSpec(memory_space=pltpu.VMEM)] * 3,
        scratch_shapes=[pltpu.SemaphoreType.DMA((6,))],
        compiler_params=pltpu.CompilerParams(vmem_limit_bytes=2 * 1024 * 1024),
        cost_estimate=pl.CostEstimate(
            flops=6 * units * width * 2048,
            transcendentals=0,
            bytes_accessed=12 * units * width,
        ),
        name="load",
    )(*gates, *ups, *downs, *after)


def expert_kernel(sizes, targets, *refs):
    count = len(sizes)
    pieces, (gate, up, down) = refs[:count], refs[count : count + 3]
    out, rows, hidden, result, out_sem = refs[-5:]
    for index, piece in enumerate(pieces):
        rows[pl.ds(sum(sizes[:index]), sizes[index]), :] = piece[...]
    contract = (((1,), (1,)), ((), ()))
    units = gate.shape[0]
    for first in range(0, units, UNIT_CHUNK):
        span = pl.ds(first, min(UNIT_CHUNK, units - first))
        gated = lax.dot_general(
            rows[...], gate[span, :], contract, preferred_element_type=jnp.float32
        )
        upward = lax.dot_general(
            rows[...], up[span, :], contract, preferred_element_type=jnp.float32
        )
        hidden[:, span] = (jax.nn.silu(gated) * upward).astype(hidden.dtype)
    slots, width = out.shape[1:]
    out_copies = []
    for first in range(0, width, OUT_CHUNK):
        span = pl.ds(first, OUT_CHUNK)
        result[:, span] = jnp.dot(
            hidden[...], down[:, span], preferred_element_type=jnp.float32
        ).astype(result.dtype)
        done = first + OUT_CHUNK
        if done % (width // COPY_GROUPS):
            continue
        group = done * COPY_GROUPS // width - 1
        columns = pl.ds(group * (width // COPY_GROUPS), width // COPY_GROUPS)
        for block in range(sum(sizes) // slots):
            copy = pltpu.make_async_copy(
                result.at[pl.ds(block * slots, slots), columns],
                out.at[targets[block], :, columns],
                out_sem.at[group, block],
            )
            copy.start()
            out_copies.append(copy)
    for copy in out_copies:
        copy.wait()


def experts(pieces, targets, held, slots, earlier=()):
    sizes = [piece.shape[0] for piece in pieces]
    units, width = held[0].shape
    count_rows = sum(sizes)
    whole = pl.BlockSpec(memory_space=pl.ANY)
    vmem = pl.BlockSpec(memory_space=pltpu.VMEM)
    first = 1 + len(pieces) + len(held)
    return pl.pallas_call(
        lambda targets, *refs: expert_kernel(sizes, targets, *refs),
        out_shape=jax.ShapeDtypeStruct((lax.axis_size("ep"), slots, width), jnp.bfloat16),
        in_specs=[pl.BlockSpec(memory_space=pltpu.SMEM)]
        + [vmem] * (len(pieces) + len(held))
        + [whole] * len(earlier),
        out_specs=whole,
        input_output_aliases={first: 0} if earlier else {},
        scratch_shapes=[
            pltpu.VMEM((count_rows, width), jnp.bfloat16),
            pltpu.VMEM((count_rows, units), jnp.bfloat16),
            pltpu.VMEM((count_rows, width), jnp.bfloat16),
            pltpu.SemaphoreType.DMA((COPY_GROUPS, count_rows // slots)),
        ],
        compiler_params=pltpu.CompilerParams(vmem_limit_bytes=16 * 1024 * 1024),
        cost_estimate=pl.CostEstimate(
            flops=6 * count_rows * units * width,
            transcendentals=count_rows * units,
            bytes_accessed=4 * count_rows * width,
        ),
        name="experts",
    )(targets, *pieces, *held, *earlier)


def link_mask(links):
    place = {"z": 16, "y": 4, "x": 1}
    return sum(place[link[0]] * (1 if link[1] == "a" else 2) for link in links)


def block_targets():
    masks = []
    for steps in (range(4), range(4, 8)):
        for colour, (first, last) in enumerate(COLOURS):
            for crossed in steps:
                spread = [spread_links(bit, colour)[0] for bit in range(3) if crossed >> bit & 1]
                masks += [link_mask(spread + select_links(block)) for block in range(first, last)]
    chip = lax.axis_index("ep")
    own = gray(chip // 16) * 16 + gray(chip // 4 % 4) * 4 + gray(chip % 4)
    code = own ^ jnp.array(masks, jnp.int32)
    return code ^ (code >> 1 & 21)


def normalize(rows, gain):
    wide = rows.astype(jnp.float32)
    scaled = wide * lax.rsqrt(jnp.mean(wide * wide, axis=-1, keepdims=True) + 1e-06)
    return (scaled * gain).astype(jnp.bfloat16)


def state_update(drive, carried, decay_rate, frequency, log_step, in_map, out_map, skip_gain):
    count_rows, width = drive.shape
    groups, half = decay_rate.shape
    channels = width // groups
    step_size = jnp.exp(log_step)[:, None]
    magnitude = jnp.exp(-decay_rate * step_size)
    real_decay = magnitude * jnp.cos(frequency * step_size)
    imag_decay = magnitude * jnp.sin(frequency * step_size)
    denom = decay_rate * decay_rate + frequency * frequency
    real_less = real_decay - 1.0
    real_factor = (-real_less * decay_rate + imag_decay * frequency) / denom
    imag_factor = (-imag_decay * decay_rate - real_less * frequency) / denom
    grouped_drive = drive.reshape(count_rows, groups, channels)
    projected = jnp.einsum(
        "sgh,gqh->sgq", grouped_drive, in_map, preferred_element_type=jnp.float32
    )
    real_in = projected[..., :half]
    imag_in = projected[..., half:]
    real_push = real_factor * real_in - imag_factor * imag_in
    imag_push = real_factor * imag_in + imag_factor * real_in
    real_old = carried[..., :half]
    imag_old = carried[..., half:]
    real_new = real_decay * real_old - imag_decay * imag_old + real_push
    imag_new = real_decay * imag_old + imag_decay * real_old + imag_push
    joined = jnp.concatenate([real_new, -imag_new], axis=-1)
    reading = jnp.einsum("sgq,ghq->sgh", joined, out_map.astype(jnp.float32))
    total = reading.reshape(count_rows, width) + skip_gain * drive.astype(jnp.float32)
    activated = jax.nn.gelu(total).astype(jnp.bfloat16)
    return (activated, jnp.concatenate([real_new, imag_new], axis=-1))


def route_weights(route_logit):
    first = jax.nn.sigmoid(route_logit[:, 0] - route_logit[:, 1])
    second = jax.nn.sigmoid(route_logit[:, 1] - route_logit[:, 0])
    return jnp.stack([first, second], axis=1)


def per_device(
    tokens,
    carried,
    decay_rate,
    frequency,
    log_step,
    in_map,
    out_map,
    skip_gain,
    norm_gain,
    w_in,
    w_out,
    expert_gain,
    route_ids,
    route_logit,
    w_gate,
    w_up,
    w_down,
):
    count_rows, model_width = tokens.shape
    core = lax.axis_index("tp")
    slots = CAP // lax.axis_size("tp")
    normed = normalize(tokens, norm_gain)
    drive = jnp.dot(normed, w_in, preferred_element_type=jnp.float32).astype(jnp.bfloat16)
    activated, new_carried = state_update(
        drive, carried, decay_rate, frequency, log_step, in_map, out_map, skip_gain
    )
    partial_value = jnp.dot(activated, w_out, preferred_element_type=jnp.float32).astype(
        jnp.bfloat16
    )
    summed = partial_value.astype(jnp.float32) + swapped(partial_value).astype(jnp.float32)
    mixed = (tokens.astype(jnp.float32) + summed).astype(jnp.bfloat16)
    expert_in = normalize(mixed, expert_gain)
    weights = route_weights(route_logit)
    gates = (w_gate.T, swapped(w_gate.T))
    ups = (w_up.T, swapped(w_up.T))
    downs = (w_down, swapped(w_down))
    chip = lax.axis_index("ep")
    own_z, own_y = chip // (Y_SIZE * X_SIZE), chip // X_SIZE % Y_SIZE
    expert_ids = jnp.arange(EXPERTS, dtype=jnp.int32)
    differ_z, differ_y = gray(expert_ids // 2) ^ gray(own_z), expert_ids % 2 ^ (own_y >> 1)
    block_of = (differ_z & 1) * 4 + (differ_z >> 1) * 2 + differ_y
    routes_flat = route_ids.reshape(-1)
    weights_flat = weights.reshape(-1)
    onehot = (routes_flat[:, None] == expert_ids[None, :]).astype(jnp.int32)
    earlier = jnp.cumsum(onehot, axis=0) - onehot
    slot_index = jnp.sum(earlier * onehot, axis=1) - core * slots
    block = jnp.sum(block_of[None, :] * onehot, axis=1)
    held = (slot_index >= 0) & (slot_index < slots)
    row_ids = jnp.arange(EXPERTS * slots, dtype=jnp.int32)[:, None]
    sent_to = jnp.where(held, block * slots + slot_index, -1)
    position = jnp.where(held, routes_flat * slots + slot_index, -1)
    sending = (row_ids == sent_to[None, :]).astype(jnp.float32)
    placement = (row_ids == position[None, :]).astype(jnp.float32)
    per_token = sending.reshape(EXPERTS * slots, count_rows, TOP).sum(axis=2)
    packed = jnp.dot(per_token.astype(jnp.bfloat16), expert_in, preferred_element_type=jnp.float32)
    blocks = packed.astype(jnp.bfloat16).reshape(EXPERTS, slots, model_width)
    came = [blocks[0]] + [
        over_links(blocks[index], select_links(index)) for index in range(1, EXPERTS)
    ]
    near = []
    for colour, (first, last) in enumerate(COLOURS):
        rows = jnp.concatenate(came[first:last], axis=0)
        for step in range(2):
            across = over_links(rows, spread_links(step, colour))
            rows = jnp.concatenate([rows, across], axis=0)
        near.append(rows)
    held_units = loaded(gates, ups, downs, ())
    far = []
    for colour, rows in enumerate(near):
        far.append(over_links(rows, spread_links(2, colour)))
    targets = block_targets()
    half = targets.shape[0] // 2
    produced = experts(near, targets[:half], held_units, slots)
    produced = experts(far, targets[half:], held_units, slots, (produced,))
    returned = lax.all_to_all(produced, "ep", split_axis=0, concat_axis=0, tiled=True)
    new_carried = with_layout_constraint(new_carried, Layout(major_to_minor=(0, 1, 2)))
    returned, new_carried = lax.optimization_barrier((returned, new_carried))
    per_expert = returned.reshape(EXPERTS, -1, slots, model_width).astype(jnp.float32).sum(axis=1)
    per_expert = per_expert.reshape(EXPERTS * slots, model_width)
    weighing = (
        (placement * weights_flat[None, :]).reshape(EXPERTS * slots, count_rows, TOP).sum(axis=2)
    )
    expert_sum = jnp.dot(weighing.T, per_expert, preferred_element_type=jnp.float32)
    half_width = model_width // lax.axis_size("tp")
    own_sum = lax.dynamic_slice_in_dim(expert_sum, core * half_width, half_width, 1)
    other_sum = lax.dynamic_slice_in_dim(expert_sum, (1 - core) * half_width, half_width, 1)
    own_mixed = lax.dynamic_slice_in_dim(mixed, core * half_width, half_width, 1)
    new_tokens = (own_mixed.astype(jnp.float32) + (own_sum + swapped(other_sum))).astype(
        jnp.bfloat16
    )
    return (new_tokens, new_carried)


def solution(mesh):
    return jax.shard_map(
        per_device,
        mesh=mesh,
        in_specs=(
            P("ep", None),
            P("ep", "tp", None),
            P("tp", None),
            P("tp", None),
            P("tp"),
            P("tp", None, None),
            P("tp", None, None),
            P("tp"),
            P(),
            P(None, "tp"),
            P("tp", None),
            P(),
            P("ep", None),
            P("ep", None),
            P(None, ("ep", "tp")),
            P(None, ("ep", "tp")),
            P(("ep", "tp"), None),
        ),
        out_specs=(P("ep", "tp"), P("ep", "tp", None)),
        check_vma=False,
    )
```

```python
import jax
import jax.numpy as jnp
from jax import lax
from jax.experimental import pallas as pl
from jax.experimental.layout import Layout, with_layout_constraint
from jax.experimental.pallas import tpu as pltpu
from jax.sharding import PartitionSpec as P

EXPERTS = 8
TOP = 2
CAP = 16
Y_SIZE = 4
X_SIZE = 4
SELECT = ("za", "zb", "yb")
SPREAD = ("ya", "xa", "xb")
COLOURS = ((0, 2), (2, 5), (5, 8))
UNIT_CHUNK = 256
OUT_CHUNK = 512
COPY_GROUPS = 1


def gray(value):
    return value ^ (value >> 1)


def neighbour(chip, link):
    place = {"z": chip // (Y_SIZE * X_SIZE), "y": chip // X_SIZE % Y_SIZE, "x": chip % X_SIZE}
    axis, bit = link
    code = gray(place[axis]) ^ (1 if bit == "a" else 2)
    place[axis] = code ^ (code >> 1)
    return (place["z"] * Y_SIZE + place["y"]) * X_SIZE + place["x"]


def over_links(shard, links):
    pairs = []
    for chip in range(lax.axis_size("ep")):
        other = chip
        for link in links:
            other = neighbour(other, link)
        pairs += [(chip * 2 + core, other * 2 + core) for core in range(2)]
    return lax.ppermute(shard, ("ep", "tp"), pairs)


def select_links(block):
    return [link for bit, link in zip((4, 2, 1), SELECT) if block & bit]


def spread_links(step, colour):
    return [SPREAD[(step + colour) % 3]]


def swapped(shard):
    return lax.ppermute(shard, "tp", [(0, 1), (1, 0)])


def load_kernel(units, *refs):
    sources, helds, sem = refs[0:6], refs[-4:-1], refs[-1]
    copies = [
        pltpu.make_async_copy(
            source, helds[index // 2].at[pl.ds(index % 2 * units, units)], sem.at[index]
        )
        for index, source in enumerate(sources)
    ]
    for copy in copies:
        copy.start()
    for copy in copies:
        copy.wait()


def loaded(gates, ups, downs, after):
    units, width = gates[0].shape
    whole = pl.BlockSpec(memory_space=pl.ANY)
    return pl.pallas_call(
        lambda *refs: load_kernel(units, *refs),
        out_shape=[pltpu.VMEM((2 * units, width), jnp.bfloat16)] * 3,
        in_specs=[whole] * (6 + len(after)),
        out_specs=[pl.BlockSpec(memory_space=pltpu.VMEM)] * 3,
        scratch_shapes=[pltpu.SemaphoreType.DMA((6,))],
        compiler_params=pltpu.CompilerParams(vmem_limit_bytes=2 * 1024 * 1024),
        cost_estimate=pl.CostEstimate(
            flops=6 * units * width * 2048,
            transcendentals=0,
            bytes_accessed=12 * units * width,
        ),
        name="load",
    )(*gates, *ups, *downs, *after)


def expert_kernel(sizes, targets, *refs):
    count = len(sizes)
    pieces, (gate, up, down) = refs[:count], refs[count : count + 3]
    out, rows, hidden, result, out_sem = refs[-5:]
    for index, piece in enumerate(pieces):
        rows[pl.ds(sum(sizes[:index]), sizes[index]), :] = piece[...]
    contract = (((1,), (1,)), ((), ()))
    units = gate.shape[0]
    for first in range(0, units, UNIT_CHUNK):
        span = pl.ds(first, min(UNIT_CHUNK, units - first))
        gated = lax.dot_general(
            rows[...], gate[span, :], contract, preferred_element_type=jnp.float32
        )
        upward = lax.dot_general(
            rows[...], up[span, :], contract, preferred_element_type=jnp.float32
        )
        hidden[:, span] = (jax.nn.silu(gated) * upward).astype(hidden.dtype)
    slots, width = out.shape[1:]
    out_copies = []
    for first in range(0, width, OUT_CHUNK):
        span = pl.ds(first, OUT_CHUNK)
        result[:, span] = jnp.dot(
            hidden[...], down[:, span], preferred_element_type=jnp.float32
        ).astype(result.dtype)
        done = first + OUT_CHUNK
        if done % (width // COPY_GROUPS):
            continue
        group = done * COPY_GROUPS // width - 1
        columns = pl.ds(group * (width // COPY_GROUPS), width // COPY_GROUPS)
        for block in range(sum(sizes) // slots):
            copy = pltpu.make_async_copy(
                result.at[pl.ds(block * slots, slots), columns],
                out.at[targets[block], :, columns],
                out_sem.at[group, block],
            )
            copy.start()
            out_copies.append(copy)
    for copy in out_copies:
        copy.wait()


def experts(pieces, targets, held, slots, earlier=()):
    sizes = [piece.shape[0] for piece in pieces]
    units, width = held[0].shape
    count_rows = sum(sizes)
    whole = pl.BlockSpec(memory_space=pl.ANY)
    vmem = pl.BlockSpec(memory_space=pltpu.VMEM)
    first = 1 + len(pieces) + len(held)
    return pl.pallas_call(
        lambda targets, *refs: expert_kernel(sizes, targets, *refs),
        out_shape=jax.ShapeDtypeStruct((lax.axis_size("ep"), slots, width), jnp.bfloat16),
        in_specs=[pl.BlockSpec(memory_space=pltpu.SMEM)]
        + [vmem] * (len(pieces) + len(held))
        + [whole] * len(earlier),
        out_specs=whole,
        input_output_aliases={first: 0} if earlier else {},
        scratch_shapes=[
            pltpu.VMEM((count_rows, width), jnp.bfloat16),
            pltpu.VMEM((count_rows, units), jnp.bfloat16),
            pltpu.VMEM((count_rows, width), jnp.bfloat16),
            pltpu.SemaphoreType.DMA((COPY_GROUPS, count_rows // slots)),
        ],
        compiler_params=pltpu.CompilerParams(vmem_limit_bytes=16 * 1024 * 1024),
        cost_estimate=pl.CostEstimate(
            flops=6 * count_rows * units * width,
            transcendentals=count_rows * units,
            bytes_accessed=4 * count_rows * width,
        ),
        name="experts",
    )(targets, *pieces, *held, *earlier)


def link_mask(links):
    place = {"z": 16, "y": 4, "x": 1}
    return sum(place[link[0]] * (1 if link[1] == "a" else 2) for link in links)


def block_targets():
    masks = []
    for steps in (range(4), range(4, 8)):
        for colour, (first, last) in enumerate(COLOURS):
            for crossed in steps:
                spread = [spread_links(bit, colour)[0] for bit in range(3) if crossed >> bit & 1]
                masks += [link_mask(spread + select_links(block)) for block in range(first, last)]
    chip = lax.axis_index("ep")
    own = gray(chip // 16) * 16 + gray(chip // 4 % 4) * 4 + gray(chip % 4)
    code = own ^ jnp.array(masks, jnp.int32)
    return code ^ (code >> 1 & 21)


def normalize(rows, gain):
    wide = rows.astype(jnp.float32)
    scaled = wide * lax.rsqrt(jnp.mean(wide * wide, axis=-1, keepdims=True) + 1e-06)
    return (scaled * gain).astype(jnp.bfloat16)


def state_update(drive, carried, decay_rate, frequency, log_step, in_map, out_map, skip_gain):
    count_rows, width = drive.shape
    groups, half = decay_rate.shape
    channels = width // groups
    step_size = jnp.exp(log_step)[:, None]
    magnitude = jnp.exp(-decay_rate * step_size)
    real_decay = magnitude * jnp.cos(frequency * step_size)
    imag_decay = magnitude * jnp.sin(frequency * step_size)
    denom = decay_rate * decay_rate + frequency * frequency
    real_less = real_decay - 1.0
    real_factor = (-real_less * decay_rate + imag_decay * frequency) / denom
    imag_factor = (-imag_decay * decay_rate - real_less * frequency) / denom
    grouped_drive = drive.reshape(count_rows, groups, channels)
    projected = jnp.einsum(
        "sgh,gqh->sgq", grouped_drive, in_map, preferred_element_type=jnp.float32
    )
    real_in = projected[..., :half]
    imag_in = projected[..., half:]
    real_push = real_factor * real_in - imag_factor * imag_in
    imag_push = real_factor * imag_in + imag_factor * real_in
    real_old = carried[..., :half]
    imag_old = carried[..., half:]
    real_new = real_decay * real_old - imag_decay * imag_old + real_push
    imag_new = real_decay * imag_old + imag_decay * real_old + imag_push
    joined = jnp.concatenate([real_new, -imag_new], axis=-1)
    reading = jnp.einsum("sgq,ghq->sgh", joined, out_map.astype(jnp.float32))
    total = reading.reshape(count_rows, width) + skip_gain * drive.astype(jnp.float32)
    activated = jax.nn.gelu(total).astype(jnp.bfloat16)
    return (activated, jnp.concatenate([real_new, imag_new], axis=-1))


def route_weights(route_logit):
    first = jax.nn.sigmoid(route_logit[:, 0] - route_logit[:, 1])
    second = jax.nn.sigmoid(route_logit[:, 1] - route_logit[:, 0])
    return jnp.stack([first, second], axis=1)


def per_device(
    tokens,
    carried,
    decay_rate,
    frequency,
    log_step,
    in_map,
    out_map,
    skip_gain,
    norm_gain,
    w_in,
    w_out,
    expert_gain,
    route_ids,
    route_logit,
    w_gate,
    w_up,
    w_down,
):
    count_rows, model_width = tokens.shape
    core = lax.axis_index("tp")
    slots = CAP // lax.axis_size("tp")
    normed = normalize(tokens, norm_gain)
    drive = jnp.dot(normed, w_in, preferred_element_type=jnp.float32).astype(jnp.bfloat16)
    activated, new_carried = state_update(
        drive, carried, decay_rate, frequency, log_step, in_map, out_map, skip_gain
    )
    partial_value = jnp.dot(activated, w_out, preferred_element_type=jnp.float32).astype(
        jnp.bfloat16
    )
    summed = partial_value.astype(jnp.float32) + swapped(partial_value).astype(jnp.float32)
    mixed = (tokens.astype(jnp.float32) + summed).astype(jnp.bfloat16)
    expert_in = normalize(mixed, expert_gain)
    weights = route_weights(route_logit)
    gates = (w_gate.T, swapped(w_gate.T))
    ups = (w_up.T, swapped(w_up.T))
    downs = (w_down, swapped(w_down))
    chip = lax.axis_index("ep")
    own_z, own_y = chip // (Y_SIZE * X_SIZE), chip // X_SIZE % Y_SIZE
    expert_ids = jnp.arange(EXPERTS, dtype=jnp.int32)
    differ_z, differ_y = gray(expert_ids // 2) ^ gray(own_z), expert_ids % 2 ^ (own_y >> 1)
    block_of = (differ_z & 1) * 4 + (differ_z >> 1) * 2 + differ_y
    routes_flat = route_ids.reshape(-1)
    weights_flat = weights.reshape(-1)
    onehot = (routes_flat[:, None] == expert_ids[None, :]).astype(jnp.int32)
    earlier = jnp.cumsum(onehot, axis=0) - onehot
    slot_index = jnp.sum(earlier * onehot, axis=1) - core * slots
    block = jnp.sum(block_of[None, :] * onehot, axis=1)
    held = (slot_index >= 0) & (slot_index < slots)
    row_ids = jnp.arange(EXPERTS * slots, dtype=jnp.int32)[:, None]
    sent_to = jnp.where(held, block * slots + slot_index, -1)
    position = jnp.where(held, routes_flat * slots + slot_index, -1)
    sending = (row_ids == sent_to[None, :]).astype(jnp.float32)
    placement = (row_ids == position[None, :]).astype(jnp.float32)
    per_token = sending.reshape(EXPERTS * slots, count_rows, TOP).sum(axis=2)
    packed = jnp.dot(per_token.astype(jnp.bfloat16), expert_in, preferred_element_type=jnp.float32)
    blocks = packed.astype(jnp.bfloat16).reshape(EXPERTS, slots, model_width)
    came = [blocks[0]] + [
        over_links(blocks[index], select_links(index)) for index in range(1, EXPERTS)
    ]
    near = []
    for colour, (first, last) in enumerate(COLOURS):
        rows = jnp.concatenate(came[first:last], axis=0)
        for step in range(2):
            across = over_links(rows, spread_links(step, colour))
            rows = jnp.concatenate([rows, across], axis=0)
        near.append(rows)
    held_units = loaded(gates, ups, downs, near[-1:])
    far = []
    for colour, rows in enumerate(near):
        far.append(over_links(rows, spread_links(2, colour)))
    targets = block_targets()
    half = targets.shape[0] // 2
    produced = experts(near, targets[:half], held_units, slots)
    produced = experts(far, targets[half:], held_units, slots, (produced,))
    returned = lax.all_to_all(produced, "ep", split_axis=0, concat_axis=0, tiled=True)
    new_carried = with_layout_constraint(new_carried, Layout(major_to_minor=(0, 1, 2)))
    returned, new_carried = lax.optimization_barrier((returned, new_carried))
    per_expert = returned.reshape(EXPERTS, -1, slots, model_width).astype(jnp.float32).sum(axis=1)
    per_expert = per_expert.reshape(EXPERTS * slots, model_width)
    weighing = (
        (placement * weights_flat[None, :]).reshape(EXPERTS * slots, count_rows, TOP).sum(axis=2)
    )
    expert_sum = jnp.dot(weighing.T, per_expert, preferred_element_type=jnp.float32)
    half_width = model_width // lax.axis_size("tp")
    own_sum = lax.dynamic_slice_in_dim(expert_sum, core * half_width, half_width, 1)
    other_sum = lax.dynamic_slice_in_dim(expert_sum, (1 - core) * half_width, half_width, 1)
    own_mixed = lax.dynamic_slice_in_dim(mixed, core * half_width, half_width, 1)
    new_tokens = (own_mixed.astype(jnp.float32) + (own_sum + swapped(other_sum))).astype(
        jnp.bfloat16
    )
    return (new_tokens, new_carried)


def solution(mesh):
    return jax.shard_map(
        per_device,
        mesh=mesh,
        in_specs=(
            P("ep", None),
            P("ep", "tp", None),
            P("tp", None),
            P("tp", None),
            P("tp"),
            P("tp", None, None),
            P("tp", None, None),
            P("tp"),
            P(),
            P(None, "tp"),
            P("tp", None),
            P(),
            P("ep", None),
            P("ep", None),
            P(None, ("ep", "tp")),
            P(None, ("ep", "tp")),
            P(("ep", "tp"), None),
        ),
        out_specs=(P("ep", "tp"), P("ep", "tp", None)),
        check_vma=False,
    )
```
